256 devices in a mesh: fs: 32 (over z, y), tp: 8 (over x, core).
Axes of the slice: x: 4, y: 4, z: 8, core: 2. Of those that a mesh axis runs over, the one named last changes fastest.
Arguments:
- x_next: bfloat16 [6144, 2048], P(('fs', 'tp')), may hold values from -6 to 6
- x_prev: bfloat16 [6144, 2048], P(('fs', 'tp')), may hold values from -6 to 6
- grad_out: bfloat16 [6144, 2048], P(('fs', 'tp')), may hold values from -24 to 24
- gate_w: bfloat16 [2048, 2816], P('fs', 'tp'), may hold values from -0.125 to 0.125
- up_w: bfloat16 [2048, 2816], P('fs', 'tp'), may hold values from -0.125 to 0.125
- down_w: bfloat16 [2816, 2048], P('tp', 'fs'), may hold values from -0.109375 to 0.109375
- acc_gate: float32 [2048, 2816], P('fs', 'tp'), may hold values from -2.5 to 2.5
- acc_up: float32 [2048, 2816], P('fs', 'tp'), may hold values from -2.5 to 2.5
- acc_down: float32 [2816, 2048], P('tp', 'fs'), may hold values from -2.5 to 2.5
Outputs:
- out_next: bfloat16 [6144, 2048], P(('fs', 'tp'))
- saved_hidden: bfloat16 [6144, 2816], P('fs', 'tp')
- grad_input: bfloat16 [6144, 2048], P(('fs', 'tp'))
- new_gate: float32 [2048, 2816], P('fs', 'tp')
- new_up: float32 [2048, 2816], P('fs', 'tp')
- new_down: float32 [2816, 2048], P('tp', 'fs')
The draws below stay inside these ranges and needn't reach their ends.
All inputs are finite; a program needn't handle non-finite values.
Results may differ from the reference program's by a relative error of at most 0.014.
Values may be sent and summed in bfloat16 or wider, within the bound.
No kernel may reach another device: no remote copies, remote signals or barrier semaphores. Data moves between devices by JAX's collectives and lax.ppermute only.
A program may use at most 64 MiB of HBM per device.

```python
import math
import jax
import jax.numpy as jnp
from jax import lax

D = 2048
FF = 2816
TOKENS = 6144
N_TP = 8


def spiked(drawn, rng, source, target, shards_of, factor):
    owner, partner = [(jnp.arange(drawn.shape[dim]) // (drawn.shape[dim] // shards_of)).reshape([-1 if axis == dim else 1 for axis in range(drawn.ndim)]) for dim in (source, target)]
    chosen = jax.random.permutation(rng, shards_of)[partner]
    strong = (owner == chosen) | (owner == (partner + shards_of // 2) % shards_of)
    return jnp.where(strong, factor * drawn, drawn)


def block_scale(key, extent, pieces, smallest, top_value):
    def one(axis_at, shards_of):
        draws = jax.random.uniform(jax.random.fold_in(jax.random.fold_in(key, 6), axis_at), (shards_of,), jnp.float32, smallest / len(pieces), top_value / len(pieces))
        return jnp.repeat(jnp.exp(draws), extent[axis_at] // shards_of).reshape((-1,) + (1,) * (len(extent) - axis_at - 1))

    loudness = one(*pieces[0])
    for cut in pieces[1:]:
        loudness = loudness * one(*cut)
    return loudness


def centred(own_key, dims, spread, bound, pieces=(), dtype=jnp.bfloat16):
    level = block_scale(own_key, dims, pieces, -0.22, 0.18) if pieces else 1.0
    entries = jax.random.normal(own_key, dims, jnp.float32) * spread * level
    return jnp.minimum(jnp.maximum(entries, -bound), bound).astype(dtype)


def heavy_noise(rng, shape, spread, limit, pieces, heavy, kind=jnp.bfloat16):
    entries = spread * jax.random.normal(rng, shape, jnp.float32)
    if pieces:
        entries = entries * block_scale(rng, shape, pieces, -0.22, 0.18)
    return jnp.clip(spiked(entries, jax.random.fold_in(rng, 3), *heavy), -limit, limit).astype(kind)


def setup_inputs(seed: int = 0) -> dict:
    key_list = jax.random.split(jax.random.key(seed), 10)
    return {
        "x_next": centred(key_list[0], (TOKENS, D), 1.0, 6.0, ((0, 256),)),
        "x_prev": centred(key_list[1], (TOKENS, D), 1.0, 6.0, ((0, 256),)),
        "grad_out": heavy_noise(key_list[2], (TOKENS, D), 1.0, 24.0, ((0, 256),), (0, 1, 256, 6.0)),
        "gate_w": centred(key_list[3], (D, FF), D ** -0.5, 0.125, ((0, 32), (1, 8))),
        "up_w": centred(key_list[4], (D, FF), D ** -0.5, 0.125, ((0, 32), (1, 8))),
        "down_w": centred(key_list[5], (FF, D), FF ** -0.5, 0.109375, ((0, 8), (1, 32))),
        "acc_gate": centred(key_list[6], (D, FF), 0.3, 2.5, ((0, 32), (1, 8)), jnp.float32),
        "acc_up": centred(key_list[7], (D, FF), 0.3, 2.5, ((0, 32), (1, 8)), jnp.float32),
        "acc_down": centred(key_list[8], (FF, D), 0.3, 2.5, ((0, 8), (1, 32)), jnp.float32),
    }


def block_sum(make_part):
    block = FF // N_TP
    total = None
    for index in range(N_TP):
        part = make_part(index * block, block)
        rounded = lax.optimization_barrier(part.astype(jnp.bfloat16)).astype(jnp.float32)
        total = rounded if total is None else total + rounded
    return total

def reference(x_next, x_prev, grad_out, gate_w, up_w, down_w, acc_gate, acc_up, acc_down):
    gate_next = jnp.dot(x_next, gate_w, preferred_element_type=jnp.float32)
    up_next = jnp.dot(x_next, up_w, preferred_element_type=jnp.float32)
    saved_hidden = (jax.nn.silu(gate_next) * up_next).astype(jnp.bfloat16)

    def out_part(start, width):
        return jnp.dot(saved_hidden[:, start:start + width], down_w[start:start + width], preferred_element_type=jnp.float32)
    out_next = block_sum(out_part).astype(jnp.bfloat16)
    gate_prev = jnp.dot(x_prev, gate_w, preferred_element_type=jnp.float32)
    up_prev = jnp.dot(x_prev, up_w, preferred_element_type=jnp.float32)
    grad_hidden = jnp.dot(grad_out, down_w.T, preferred_element_type=jnp.float32)
    sigmoid_gate = jax.nn.sigmoid(gate_prev)
    silu_gate = gate_prev * sigmoid_gate
    grad_gate = (grad_hidden * up_prev * sigmoid_gate * (1.0 + gate_prev * (1.0 - sigmoid_gate))).astype(jnp.bfloat16)
    grad_up = (grad_hidden * silu_gate).astype(jnp.bfloat16)
    hidden_prev = (silu_gate * up_prev).astype(jnp.bfloat16)

    def input_part(start, width):
        first = jnp.dot(grad_gate[:, start:start + width], gate_w[:, start:start + width].T, preferred_element_type=jnp.float32)
        second = jnp.dot(grad_up[:, start:start + width], up_w[:, start:start + width].T, preferred_element_type=jnp.float32)
        return first + second
    grad_input = block_sum(input_part).astype(jnp.bfloat16)
    factor = 1.0 / math.sqrt(TOKENS)
    new_gate = acc_gate + factor * jnp.dot(x_prev.T, grad_gate, preferred_element_type=jnp.float32)
    new_up = acc_up + factor * jnp.dot(x_prev.T, grad_up, preferred_element_type=jnp.float32)
    new_down = acc_down + factor * jnp.dot(hidden_prev.T, grad_out, preferred_element_type=jnp.float32)
    return (out_next, saved_hidden, grad_input, new_gate, new_up, new_down)
```

```python
import math

import jax
import jax.numpy as jnp
from jax import lax
from jax.sharding import Mesh
from jax.sharding import PartitionSpec as P


BF16 = jnp.bfloat16
F32 = jnp.float32
FS = ("z", "y")
TP = ("x", "c")
ALL = ("z", "y", "x", "c")
PLANE = ("y", "x")


def spread(blocks, axis):
    return lax.all_to_all(blocks, axis, 0, 0, tiled=True)


def gathered(array, axis):
    return spread(jnp.broadcast_to(array[None], (lax.axis_size(axis), *array.shape)), axis)


def swapped(array):
    return lax.ppermute(array, "c", [(0, 1), (1, 0)])


def dot(left, right, dims):
    return lax.dot_general(left, right, (dims, ((), ())), preferred_element_type=F32)


def local(x_next, x_prev, grad_out, gate_w, up_w, down_w, acc_gate, acc_up, acc_down):
    rows, width = x_prev.shape
    nz, ny, nx, nc = (lax.axis_size(name) for name in ALL)
    plane = ny * nx
    total_rows = rows * nz * ny * nx * nc
    factor = 1.0 / math.sqrt(total_rows)
    units = gate_w.shape[1]
    part = units // ny
    shard = gate_w.shape[0]
    deep = shard * ny
    core = lax.axis_index("c")

    mine = jnp.stack((gate_w.T, up_w.T, down_w)).reshape(3, ny, part, shard)
    mine = spread(jnp.moveaxis(mine, 1, 0), "y")
    mine = jnp.moveaxis(mine, 0, 2).reshape(3, part, deep)
    own = gathered(mine, "z")
    other = swapped(own)
    weights = jnp.stack((own, other))
    weights = weights.transpose(2, 0, 3, 1, 4).reshape(3, 2 * part, width)
    gate_up = weights[:2].reshape(4 * part, width)
    down = weights[2]

    both = gathered(jnp.concatenate((x_prev, grad_out), axis=1), PLANE).reshape(plane * rows, 2 * width)
    prev, cotangent = both[:, :width], both[:, width:]
    later = gathered(x_next, PLANE).reshape(plane * rows, width)

    pre = dot(prev, gate_up, ((1,), (1,)))
    gate_prev, up_prev = pre[:, : 2 * part], pre[:, 2 * part :]
    grad_hidden = dot(cotangent, down, ((1,), (1,)))
    sig = jax.nn.sigmoid(gate_prev)
    silu = gate_prev * sig
    grad_gate = (grad_hidden * up_prev * sig * (1.0 + gate_prev * (1.0 - sig))).astype(BF16)
    grad_up = (grad_hidden * silu).astype(BF16)
    hidden_prev = (silu * up_prev).astype(BF16)
    grads = jnp.concatenate((grad_gate, grad_up), axis=1)
    term = dot(grads, prev, ((0,), (0,))).reshape(2, 2, part, width)
    term_down = dot(hidden_prev, cotangent, ((0,), (0,))).reshape(1, 2, part, width)
    kept = jnp.concatenate((term[:, 0], term_down[:, 0]))
    sent = jnp.concatenate((term[:, 1], term_down[:, 1])).astype(BF16)
    paired = (kept + swapped(sent).astype(F32)).astype(BF16)
    paired = jnp.moveaxis(paired.reshape(3, part, nz, deep), 2, 0)
    summed = jnp.sum(spread(paired, "z").astype(F32), axis=0).astype(BF16)
    summed = jnp.moveaxis(summed.reshape(3, part, ny, shard), 2, 0)
    summed = jnp.moveaxis(spread(summed, "y"), 0, 1).reshape(3, units, shard).astype(F32)
    new_gate = acc_gate + factor * summed[0].T
    new_up = acc_up + factor * summed[1].T
    new_down = acc_down + factor * summed[2]

    input_part = dot(grads, gate_up, ((1,), (0,))).astype(BF16).reshape(plane, rows, width)
    grad_input = jnp.sum(spread(input_part, PLANE).astype(F32), axis=0).astype(BF16)

    pre_next = dot(later, gate_up, ((1,), (1,)))
    hidden = (jax.nn.silu(pre_next[:, : 2 * part]) * pre_next[:, 2 * part :]).astype(BF16)
    out_part = dot(hidden, down, ((1,), (0,))).astype(BF16).reshape(plane, rows, width)
    out_next = jnp.sum(spread(out_part, PLANE).astype(F32), axis=0).astype(BF16)

    halves = hidden.reshape(ny, nx * rows, 2, part)
    first, second = halves[:, :, 0], halves[:, :, 1]
    low = jnp.where(core == 0, first, second)
    high = jnp.where(core == 0, second, first)
    saved = spread(jnp.stack((low, high), axis=1).reshape(ny * nc, nx * rows, part), ("y", "c"))
    saved = saved.reshape(ny, nc, nx, rows, part).transpose(2, 1, 3, 0, 4)
    saved = saved.reshape(nx * nc * rows, units)
    return out_next, saved, grad_input, new_gate, new_up, new_down


def solution(mesh):
    split = Mesh(mesh.devices.reshape(8, 4, 4, 2), ALL)
    tokens = P(ALL, None)
    wide, tall = P(FS, TP), P(TP, FS)
    in_specs = (tokens, tokens, tokens, wide, wide, tall, wide, wide, tall)
    out_specs = (tokens, wide, tokens, wide, wide, tall)
    return jax.shard_map(local, mesh=split, in_specs=in_specs, out_specs=out_specs, check_vma=False)
```

```python
import math

import jax
import jax.numpy as jnp
from jax import lax
from jax.sharding import Mesh
from jax.sharding import PartitionSpec as P


BF16 = jnp.bfloat16
F32 = jnp.float32
FS = ("z", "y")
TP = ("x", "c")
ALL = ("z", "y", "x", "c")


def spread(blocks, axis):
    return lax.all_to_all(blocks, axis, 0, 0, tiled=True)


def gathered(array, axis):
    return spread(jnp.broadcast_to(array[None], (lax.axis_size(axis), *array.shape)), axis)


def swapped(array):
    return lax.ppermute(array, "c", [(0, 1), (1, 0)])


def moved(array, axis, step):
    length = lax.axis_size(axis)
    return lax.ppermute(array, axis, [(i, (i + step) % length) for i in range(length)])


def around(array, axis):
    return [array] + [moved(array, axis, -step) for step in range(1, lax.axis_size(axis))]


def sum_for_owner(blocks, axis):
    total = blocks[0].astype(F32)
    for step in range(1, len(blocks)):
        total = total + moved(blocks[step], axis, step).astype(F32)
    return total.astype(BF16)


def dot(left, right, dims):
    return lax.dot_general(left, right, (dims, ((), ())), preferred_element_type=F32)


def local(x_next, x_prev, grad_out, gate_w, up_w, down_w, acc_gate, acc_up, acc_down):
    rows, width = x_prev.shape
    nz, ny, nx, nc = (lax.axis_size(name) for name in ALL)
    plane = ny * nx
    total_rows = rows * nz * ny * nx * nc
    factor = 1.0 / math.sqrt(total_rows)
    units = gate_w.shape[1]
    part = units // ny
    shard = gate_w.shape[0]
    deep = shard * ny
    core = lax.axis_index("c")

    mine = jnp.stack((gate_w.T, up_w.T, down_w)).reshape(3, ny, part, shard)
    mine = spread(jnp.moveaxis(mine, 1, 0), "y")
    mine = jnp.moveaxis(mine, 0, 2).reshape(3, part, deep)
    own = gathered(mine, "z")
    other = swapped(own)
    weights = jnp.stack((own, other))
    weights = weights.transpose(2, 0, 3, 1, 4).reshape(3, 2 * part, width)
    gate_up = weights[:2].reshape(4 * part, width)
    down = weights[2]

    half = width // 2
    first = jnp.concatenate((x_prev, x_next[:, :half]), axis=1)
    second = jnp.concatenate((grad_out, x_next[:, half:]), axis=1)
    first = jnp.stack(around(first, "x"))
    second = jnp.stack(around(second, "y"))
    first = jnp.stack(around(first, "y"))
    second = jnp.stack(around(second, "x"), axis=1)
    first = first.reshape(plane * rows, width + half)
    second = second.reshape(plane * rows, width + half)
    prev, cotangent = first[:, :width], second[:, :width]
    later = jnp.concatenate((first[:, width:], second[:, width:]), axis=1)

    pre = dot(prev, gate_up, ((1,), (1,)))
    gate_prev, up_prev = pre[:, : 2 * part], pre[:, 2 * part :]
    grad_hidden = dot(cotangent, down, ((1,), (1,)))
    sig = jax.nn.sigmoid(gate_prev)
    silu = gate_prev * sig
    grad_gate = (grad_hidden * up_prev * sig * (1.0 + gate_prev * (1.0 - sig))).astype(BF16)
    grad_up = (grad_hidden * silu).astype(BF16)
    hidden_prev = (silu * up_prev).astype(BF16)
    grads = jnp.concatenate((grad_gate, grad_up), axis=1)
    term = dot(grads, prev, ((0,), (0,))).reshape(2, 2, part, width)
    term_down = dot(hidden_prev, cotangent, ((0,), (0,))).reshape(1, 2, part, width)
    kept = jnp.concatenate((term[:, 0], term_down[:, 0]))
    sent = jnp.concatenate((term[:, 1], term_down[:, 1])).astype(BF16)
    paired = (kept + swapped(sent).astype(F32)).astype(BF16)
    paired = jnp.moveaxis(paired.reshape(3, part, nz, deep), 2, 0)
    summed = jnp.sum(spread(paired, "z").astype(F32), axis=0).astype(BF16)
    summed = jnp.moveaxis(summed.reshape(3, part, ny, shard), 2, 0)
    summed = jnp.moveaxis(spread(summed, "y"), 0, 1).reshape(3, units, shard).astype(F32)
    new_gate = acc_gate + factor * summed[0].T
    new_up = acc_up + factor * summed[1].T
    new_down = acc_down + factor * summed[2]

    input_part = dot(grads, gate_up, ((1,), (0,))).astype(BF16).reshape(ny, nx, rows, width)
    by_x = sum_for_owner([input_part[:, k] for k in range(nx)], "x")
    grad_input = sum_for_owner([by_x[k] for k in range(ny)], "y")

    pre_next = dot(later, gate_up, ((1,), (1,)))
    hidden = (jax.nn.silu(pre_next[:, : 2 * part]) * pre_next[:, 2 * part :]).astype(BF16)
    out_part = dot(hidden, down, ((1,), (0,))).astype(BF16).reshape(ny, nx, rows, width)
    by_y = sum_for_owner([out_part[k] for k in range(ny)], "y")
    out_next = sum_for_owner([by_y[k] for k in range(nx)], "x")

    ordered = hidden.reshape(ny, nx, rows, 2, part)
    ordered = jnp.roll(ordered, (lax.axis_index("y"), lax.axis_index("x")), (0, 1))
    halves = ordered.reshape(ny, nx * rows, 2, part)
    ahead, behind = halves[:, :, 0], halves[:, :, 1]
    low = jnp.where(core == 0, ahead, behind)
    high = jnp.where(core == 0, behind, ahead)
    saved = spread(jnp.stack((low, high), axis=1).reshape(ny * nc, nx * rows, part), ("y", "c"))
    saved = saved.reshape(ny, nc, nx, rows, part).transpose(2, 1, 3, 0, 4)
    saved = saved.reshape(nx * nc * rows, units)
    return out_next, saved, grad_input, new_gate, new_up, new_down


def solution(mesh):
    split = Mesh(mesh.devices.reshape(8, 4, 4, 2), ALL)
    tokens = P(ALL, None)
    wide, tall = P(FS, TP), P(TP, FS)
    in_specs = (tokens, tokens, tokens, wide, wide, tall, wide, wide, tall)
    out_specs = (tokens, wide, tokens, wide, wide, tall)
    return jax.shard_map(local, mesh=split, in_specs=in_specs, out_specs=out_specs, check_vma=False)
```

```python
import math

import jax
import jax.numpy as jnp
from jax import lax
from jax.sharding import Mesh
from jax.sharding import PartitionSpec as P


BF16 = jnp.bfloat16
F32 = jnp.float32
FS = ("z", "y")
TP = ("x", "c")
ALL = ("z", "y", "x", "c")


def spread(blocks, axis):
    return lax.all_to_all(blocks, axis, 0, 0, tiled=True)


def gathered(array, axis):
    return spread(jnp.broadcast_to(array[None], (lax.axis_size(axis), *array.shape)), axis)


def swapped(array):
    return lax.ppermute(array, "c", [(0, 1), (1, 0)])


def moved(array, axis, step):
    length = lax.axis_size(axis)
    return lax.ppermute(array, axis, [(i, (i + step) % length) for i in range(length)])


def around(array, axis):
    return [array] + [moved(array, axis, -step) for step in range(1, lax.axis_size(axis))]


def sum_for_owner(blocks, axis):
    total = blocks[0].astype(F32)
    for step in range(1, len(blocks)):
        total = total + moved(blocks[step], axis, step).astype(F32)
    return total.astype(BF16)


def dot(left, right, dims):
    return lax.dot_general(left, right, (dims, ((), ())), preferred_element_type=F32)


def layer(x_next, x_prev, grad_out, gate_w, up_w, down_w, acc_gate, acc_up, acc_down):
    rows, width = x_prev.shape
    nz, ny, nx, nc = (lax.axis_size(name) for name in ALL)
    plane = ny * nx
    total_rows = rows * nz * ny * nx * nc
    factor = 1.0 / math.sqrt(total_rows)
    units = gate_w.shape[1]
    part = units // ny
    shard = gate_w.shape[0]
    deep = shard * ny
    core = lax.axis_index("c")

    half = width // 2
    first = jnp.concatenate((x_prev, x_next[:, :half]), axis=1)
    second = jnp.concatenate((grad_out, x_next[:, half:]), axis=1)
    first = around(first, "x")
    second = around(second, "y")
    first, second = jnp.stack(first), jnp.stack(second)
    first = around(first, "y")
    second = around(second, "x")
    first = jnp.stack(first).reshape(plane * rows, width + half)
    second = jnp.stack(second, axis=1).reshape(plane * rows, width + half)
    prev, cotangent = first[:, :width], second[:, :width]
    later = jnp.concatenate((first[:, width:], second[:, width:]), axis=1)

    mine = jnp.stack((gate_w.T, up_w.T, down_w)).reshape(3, ny, part, shard)
    mine = jnp.moveaxis(mine, 1, 0)
    mine = spread(mine, "y")
    mine = jnp.moveaxis(mine, 0, 2).reshape(3, part, deep)
    own = gathered(mine, "z")
    other = swapped(own)
    weights = jnp.stack((own, other))
    weights = weights.transpose(2, 0, 3, 1, 4).reshape(3, 2 * part, width)
    gate_up = weights[:2].reshape(4 * part, width)
    down = weights[2]

    pre = dot(prev, gate_up, ((1,), (1,)))
    gate_prev, up_prev = pre[:, : 2 * part], pre[:, 2 * part :]
    grad_hidden = dot(cotangent, down, ((1,), (1,)))
    sig = jax.nn.sigmoid(gate_prev)
    silu = gate_prev * sig
    grad_gate = (grad_hidden * up_prev * sig * (1.0 + gate_prev * (1.0 - sig))).astype(BF16)
    grad_up = (grad_hidden * silu).astype(BF16)
    hidden_prev = (silu * up_prev).astype(BF16)
    grads = jnp.concatenate((grad_gate, grad_up), axis=1)
    term = dot(grads, prev, ((0,), (0,))).reshape(2, 2, part, width)
    term_down = dot(hidden_prev, cotangent, ((0,), (0,))).reshape(1, 2, part, width)
    kept = jnp.concatenate((term[:, 0], term_down[:, 0]))
    sent = jnp.concatenate((term[:, 1], term_down[:, 1])).astype(BF16)
    sent = swapped(sent)
    paired = (kept + sent.astype(F32)).astype(BF16)
    paired = jnp.moveaxis(paired.reshape(3, part, nz, deep), 2, 0)
    summed = spread(paired, "z")
    summed = jnp.sum(summed.astype(F32), axis=0).astype(BF16)
    summed = jnp.moveaxis(summed.reshape(3, part, ny, shard), 2, 0)
    summed = spread(summed, "y")
    summed = jnp.moveaxis(summed, 0, 1).reshape(3, units, shard).astype(F32)
    new_gate = acc_gate + factor * summed[0].T
    new_up = acc_up + factor * summed[1].T
    new_down = acc_down + factor * summed[2]

    input_part = dot(grads, gate_up, ((1,), (0,))).astype(BF16).reshape(ny, nx, rows, width)
    by_x = sum_for_owner([input_part[:, k] for k in range(nx)], "x")
    grad_input = sum_for_owner([by_x[k] for k in range(ny)], "y")

    pre_next = dot(later, gate_up, ((1,), (1,)))
    hidden = (jax.nn.silu(pre_next[:, : 2 * part]) * pre_next[:, 2 * part :]).astype(BF16)
    out_part = dot(hidden, down, ((1,), (0,))).astype(BF16).reshape(ny, nx, rows, width)
    by_y = sum_for_owner([out_part[k] for k in range(ny)], "y")
    out_next = sum_for_owner([by_y[k] for k in range(nx)], "x")

    partner = swapped(hidden[:, part:])
    pair = jnp.stack((hidden[:, :part], partner)).reshape(nc, ny, nx, rows, part)
    back = [pair[:, 0]] + [moved(pair[:, step], "y", step) for step in range(1, ny)]
    saved = jnp.stack([back[-step % ny] for step in range(ny)])
    saved = jnp.roll(saved, (lax.axis_index("y"), lax.axis_index("x")), (0, 2))
    saved = jnp.where(core == 0, saved, saved[:, ::-1])
    saved = saved.transpose(2, 1, 3, 0, 4).reshape(nx * nc * rows, units)
    return out_next, saved, grad_input, new_gate, new_up, new_down


def solution(mesh):
    split = Mesh(mesh.devices.reshape(8, 4, 4, 2), ALL)
    tokens = P(ALL, None)
    wide, tall = P(FS, TP), P(TP, FS)
    in_specs = (tokens, tokens, tokens, wide, wide, tall, wide, wide, tall)
    out_specs = (tokens, wide, tokens, wide, wide, tall)
    return jax.shard_map(layer, mesh=split, in_specs=in_specs, out_specs=out_specs, check_vma=False)
```

```python
import functools
import math

import jax
import jax.numpy as jnp
from jax import lax
from jax.experimental import pallas as pl
from jax.experimental.pallas import tpu as pltpu
from jax.sharding import Mesh
from jax.sharding import PartitionSpec as P


BF16 = jnp.bfloat16
F32 = jnp.float32
FS = ("z", "y")
TP = ("x", "c")
ALL = ("z", "y", "x", "c")


def spread(blocks, axis):
    return lax.all_to_all(blocks, axis, 0, 0, tiled=True)


def swapped(array):
    return lax.ppermute(array, "c", [(0, 1), (1, 0)])


def moved(array, axis, step):
    length = lax.axis_size(axis)
    return lax.ppermute(array, axis, [(i, (i + step) % length) for i in range(length)])


def around(array, axis):
    return [array] + [moved(array, axis, -step) for step in range(1, lax.axis_size(axis))]


def sum_for_owner(blocks, axis):
    total = blocks[0].astype(F32)
    for step in range(1, len(blocks)):
        total = total + moved(blocks[step], axis, step).astype(F32)
    return total.astype(BF16)


def dot(left, right, dims):
    return lax.dot_general(left, right, (dims, ((), ())), preferred_element_type=F32)


LANES = 128


def whole(kernel, out_shape, scratch=(), flops=0, moved_bytes=0):
    return pl.pallas_call(
        kernel,
        out_shape=out_shape,
        scratch_shapes=scratch,
        cost_estimate=pl.CostEstimate(flops=flops, bytes_accessed=moved_bytes, transcendentals=0),
    )


def like(shape, kind):
    return jax.ShapeDtypeStruct(shape, kind)


def exchange_lanes(left, right):
    half = LANES // 2
    lane = lax.broadcasted_iota(jnp.int32, left.shape, 1)
    low = jnp.where(lane < half, left, pltpu.roll(right, half, 1))
    high = jnp.where(lane < half, pltpu.roll(left, half, 1), right)
    return low, high


def pack_kernel(copies, part, pad, gate, up, down, out):
    both = jnp.concatenate((gate[...], up[...]), axis=0).astype(F32).T
    tall = down[...].astype(F32)
    half = pad // 2
    shard = tall.shape[1]
    for y in range(tall.shape[0] // part):
        top = both[y * part : (y + 1) * part]
        piece = tall[y * part : (y + 1) * part]
        first, second = piece[:half], piece[half:]
        second = jnp.concatenate((second, jnp.zeros((pad - part, shard), F32)))
        low = jnp.concatenate((first, second), axis=1)
        block = jnp.concatenate((top, jnp.zeros((pad - part, LANES), F32), low)).astype(BF16)
        for z in range(copies):
            out[z * (tall.shape[0] // part) + y] = block


def turned(array, outer, inner, rows):
    return jnp.concatenate(
        [
            array[(o * inner + i) * rows : (o * inner + i + 1) * rows]
            for i in range(inner)
            for o in range(outer)
        ]
    )


def backward_kernel(ny, nx, rows, pad, own, other, *refs):
    firsts, seconds = refs[:ny], refs[ny : ny + nx]
    kept, sent, gate_up, down, grads, prev, cotangent = refs[ny + nx :]
    width = prev.shape[1]
    half = pad // 2
    for base, packed in ((0, own), (pad, other)):
        for tile in range(packed.shape[0] // 2):
            at = pl.ds(tile * LANES, LANES)
            low, high = exchange_lanes(packed[2 * tile].astype(F32), packed[2 * tile + 1].astype(F32))
            gate_up[pl.ds(base, pad), at] = low[:pad].astype(BF16)
            gate_up[pl.ds(2 * pad + base, pad), at] = high[:pad].astype(BF16)
            down[pl.ds(base, half), at] = low[pad:].astype(BF16)
            down[pl.ds(base + half, half), at] = high[pad:].astype(BF16)
    for k in range(ny):
        prev[pl.ds(k * nx * rows, nx * rows)] = firsts[k][:, :width]
    for k in range(nx):
        cotangent[pl.ds(k * ny * rows, ny * rows)] = seconds[k][:, :width]
    pre = dot(prev[...], gate_up[...], ((1,), (1,)))
    gate_prev, up_prev = pre[:, : 2 * pad], pre[:, 2 * pad :]
    grad_hidden = turned(dot(cotangent[...], down[...], ((1,), (1,))), nx, ny, rows)
    sig = jax.nn.sigmoid(gate_prev)
    silu = gate_prev * sig
    grad_gate = grad_hidden * up_prev * sig * (1.0 + gate_prev * (1.0 - sig))
    grad_up = grad_hidden * silu
    hidden_prev = turned(silu * up_prev, ny, nx, rows)
    grads[:, : 2 * pad] = grad_gate.astype(BF16)
    grads[:, 2 * pad :] = grad_up.astype(BF16)
    for k, (value, tokens) in enumerate(((grad_gate, prev), (grad_up, prev), (hidden_prev, cotangent))):
        term = dot(value.astype(BF16).T, tokens[...], ((1,), (0,)))
        kept[pl.ds(k * pad, pad)] = term[:pad]
        sent[pl.ds(k * pad, pad)] = term[pad:].astype(BF16)


def pair_kernel(pad, kept, received, out):
    half = pad // 2
    for tile in range(out.shape[0] // 2):
        at = pl.ds(tile * LANES, LANES)
        total = kept[:, at] + received[:, at].astype(F32)
        left = jnp.concatenate((total[:pad], total[2 * pad : 2 * pad + half]))
        right = jnp.concatenate((total[pad : 2 * pad], total[2 * pad + half :]))
        even, odd = exchange_lanes(left, right)
        out[2 * tile] = even.astype(BF16)
        out[2 * tile + 1] = odd.astype(BF16)


def update_kernel(ny, part, pad, factor, arrived, gate, up, down, new_gate, new_up, new_down):
    half = pad // 2
    shard = down.shape[1]
    tops = []
    for y in range(ny):
        total = arrived[y].astype(F32)
        for z in range(1, arrived.shape[0] // ny):
            total = total + arrived[z * ny + y].astype(F32)
        tops.append(total[:part])
        low = total[pad:]
        high = pltpu.roll(low, LANES // 2, 1)
        at = y * part
        new_down[at : at + half] = down[at : at + half] + factor * low[:, :shard]
        rest = part - half
        new_down[at + half : at + part] = down[at + half : at + part] + factor * high[:rest, :shard]
    both = jnp.concatenate(tops).T
    new_gate[...] = gate[...] + factor * both[:shard]
    new_up[...] = up[...] + factor * both[shard:]


def forward_kernel(ny, nx, rows, pad, gate_up, down, *refs):
    firsts, seconds = refs[:ny], refs[ny : ny + nx]
    hidden, outs, tokens = refs[ny + nx], refs[ny + nx + 1 : -1], refs[-1]
    half = tokens.shape[1]
    width = gate_up.shape[1]
    for k in range(ny):
        tokens[pl.ds(k * nx * rows, nx * rows)] = firsts[k][:, width:]
    pre = dot(tokens[...], gate_up[:, :half], ((1,), (1,)))
    for k in range(nx):
        tokens[pl.ds(k * ny * rows, ny * rows)] = seconds[k][:, width:]
    pre = pre + turned(dot(tokens[...], gate_up[:, half:], ((1,), (1,))), nx, ny, rows)
    value = (jax.nn.silu(pre[:, : 2 * pad]) * pre[:, 2 * pad :]).astype(BF16)
    hidden[...] = value
    total = dot(value, down[...], ((1,), (0,)))
    for k in range(ny):
        outs[k][...] = total[k * nx * rows : (k + 1) * nx * rows].astype(BF16)


def layer(x_next, x_prev, grad_out, gate_w, up_w, down_w, acc_gate, acc_up, acc_down):
    rows, width = x_prev.shape
    nz, ny, nx, nc = (lax.axis_size(name) for name in ALL)
    group = ny * nx * rows
    factor = 1.0 / math.sqrt(rows * nz * ny * nx * nc)
    _, units = gate_w.shape
    part = units // ny
    pad = -(-part // 32) * 32
    tall = pad + pad // 2
    core = lax.axis_index("c")

    half = width // 2
    first = jnp.concatenate((x_prev, x_next[:, :half]), axis=1)
    second = jnp.concatenate((grad_out, x_next[:, half:]), axis=1)
    first = around(first, "x")
    second = around(second, "y")
    first = jnp.stack(first).reshape(nx * rows, width + half)
    second = jnp.stack(second).reshape(ny * rows, width + half)
    firsts = around(first, "y")
    seconds = around(second, "x")

    packed = whole(
        functools.partial(pack_kernel, nz, part, pad), like((nz * ny, tall, LANES), BF16)
    )(gate_w, up_w, down_w)
    own = spread(packed, FS)
    other = swapped(own)

    token_ops = 2 * group * 2 * pad * width
    kept, sent, gate_up, down, grads = whole(
        functools.partial(backward_kernel, ny, nx, rows, pad),
        (
            like((3 * pad, width), F32),
            like((3 * pad, width), BF16),
            like((4 * pad, width), BF16),
            like((2 * pad, width), BF16),
            like((group, 4 * pad), BF16),
        ),
        (pltpu.VMEM((group, width), BF16), pltpu.VMEM((group, width), BF16)),
        flops=6 * token_ops,
        moved_bytes=12 * group * width,
    )(own, other, *firsts, *seconds)
    received = swapped(sent)
    paired = whole(
        functools.partial(pair_kernel, pad), like((nz * ny, tall, LANES), BF16)
    )(kept, received)
    arrived = spread(paired, FS)
    new_gate, new_up, new_down = whole(
        functools.partial(update_kernel, ny, part, pad, factor),
        (like(acc_gate.shape, F32), like(acc_up.shape, F32), like(acc_down.shape, F32)),
    )(arrived, acc_gate, acc_up, acc_down)

    input_part = dot(grads, gate_up, ((1,), (0,))).astype(BF16).reshape(ny, nx, rows, width)
    by_x = sum_for_owner([input_part[:, k] for k in range(nx)], "x")
    grad_input = sum_for_owner([by_x[k] for k in range(ny)], "y")

    hidden, *out_part = whole(
        functools.partial(forward_kernel, ny, nx, rows, pad),
        (like((group, 2 * pad), BF16), *(like((nx * rows, width), BF16) for _ in range(ny))),
        (pltpu.VMEM((group, half), BF16),),
        flops=3 * token_ops,
        moved_bytes=6 * group * width,
    )(gate_up, down, *firsts, *seconds)
    by_y = sum_for_owner(out_part, "y").reshape(nx, rows, width)
    out_next = sum_for_owner([by_y[k] for k in range(nx)], "x")

    partner = swapped(hidden[:, pad : pad + part])
    pair = jnp.stack((hidden[:, :part], partner)).reshape(nc, ny, nx, rows, part)
    back = [pair[:, 0]] + [moved(pair[:, step], "y", step) for step in range(1, ny)]
    saved = jnp.stack([back[-step % ny] for step in range(ny)])
    saved = jnp.roll(saved, (lax.axis_index("y"), lax.axis_index("x")), (0, 2))
    saved = jnp.where(core == 0, saved, saved[:, ::-1])
    saved = saved.transpose(2, 1, 3, 0, 4).reshape(nx * nc * rows, units)
    return out_next, saved, grad_input, new_gate, new_up, new_down


def solution(mesh):
    split = Mesh(mesh.devices.reshape(8, 4, 4, 2), ALL)
    tokens = P(ALL, None)
    wide, tall = P(FS, TP), P(TP, FS)
    in_specs = (tokens, tokens, tokens, wide, wide, tall, wide, wide, tall)
    out_specs = (tokens, wide, tokens, wide, wide, tall)
    return jax.shard_map(layer, mesh=split, in_specs=in_specs, out_specs=out_specs, check_vma=False)
```

```python
import functools
import math

import jax
import jax.numpy as jnp
from jax import lax
from jax.experimental import pallas as pl
from jax.experimental.pallas import tpu as pltpu
from jax.sharding import Mesh
from jax.sharding import PartitionSpec as P


BF16 = jnp.bfloat16
F32 = jnp.float32
FS = ("z", "y")
TP = ("x", "c")
ALL = ("z", "y", "x", "c")


def spread(blocks, axis):
    return lax.all_to_all(blocks, axis, 0, 0, tiled=True)


def swapped(array):
    return lax.ppermute(array, "c", [(0, 1), (1, 0)])


def moved(array, axis, step):
    length = lax.axis_size(axis)
    return lax.ppermute(array, axis, [(i, (i + step) % length) for i in range(length)])


def around(array, axis):
    return [array] + [moved(array, axis, -step) for step in range(1, lax.axis_size(axis))]


def for_owner(blocks, axis):
    return [blocks[0]] + [moved(blocks[step], axis, step) for step in range(1, len(blocks))]


def added(parts):
    total = parts[0].astype(F32)
    for part in parts[1:]:
        total = total + part.astype(F32)
    return total.astype(BF16)


def dot(left, right, dims):
    return lax.dot_general(left, right, (dims, ((), ())), preferred_element_type=F32)


LANES = 128


def whole(kernel, out_shape, inputs, scratch=(), flops=0, grant=12, scalars=0):
    spec = pl.BlockSpec(memory_space=pltpu.VMEM)
    count = len(inputs) - scalars
    single = not isinstance(out_shape, tuple)
    return pl.pallas_call(
        kernel,
        out_shape=out_shape,
        in_specs=[pl.BlockSpec(memory_space=pltpu.SMEM)] * scalars + [spec] * count,
        out_specs=spec if single else tuple(spec for _ in out_shape),
        scratch_shapes=scratch,
        compiler_params=pltpu.CompilerParams(vmem_limit_bytes=grant * 2**20),
        cost_estimate=pl.CostEstimate(flops=flops, bytes_accessed=0, transcendentals=0),
    )(*inputs)


def like(shape, kind):
    return jax.ShapeDtypeStruct(shape, kind)


def exchange_lanes(left, right):
    half = LANES // 2
    lane = lax.broadcasted_iota(jnp.int32, left.shape, 1)
    low = jnp.where(lane < half, left, pltpu.roll(right, half, 1))
    high = jnp.where(lane < half, pltpu.roll(left, half, 1), right)
    return low, high


def front_kernel(copies, part, pad, x_next, x_prev, grad_out, gate, up, down_t, first, second, out):
    width = x_prev.shape[1]
    mid = width // 2
    first[:, :width] = x_prev[...]
    first[:, width:] = x_next[:, :mid]
    second[:, :width] = grad_out[...]
    second[:, width:] = x_next[:, mid:]
    shard, units = gate.shape
    both = jnp.concatenate((gate[...], up[...]), axis=0).astype(F32).T
    tall = jnp.concatenate((down_t[...], jnp.zeros_like(down_t))).astype(F32).T[:, :shard]
    half = pad // 2
    count = units // part
    for y in range(count):
        top = both[y * part : (y + 1) * part]
        piece = tall[y * part : (y + 1) * part]
        ahead, behind = piece[:half], piece[half:]
        behind = jnp.concatenate((behind, jnp.zeros((pad - part, shard), F32)))
        low = jnp.concatenate((ahead, behind), axis=1)
        block = jnp.concatenate((top, jnp.zeros((pad - part, LANES), F32), low)).astype(BF16)
        for z in range(copies):
            out[z * count + y] = block


def turned(array, outer, inner, rows):
    return jnp.concatenate(
        [
            array[(o * inner + i) * rows : (o * inner + i + 1) * rows]
            for i in range(inner)
            for o in range(outer)
        ]
    )


def backward_kernel(ny, nx, rows, pad, own, other, *refs):
    firsts, seconds = refs[:ny], refs[ny : ny + nx]
    kept, sent, gate_up, down, grads, prev, cotangent = refs[ny + nx :]
    half = pad // 2
    for base, packed in ((0, own), (pad, other)):
        for tile in range(packed.shape[0] // 2):
            at = pl.ds(tile * LANES, LANES)
            low, high = exchange_lanes(packed[2 * tile].astype(F32), packed[2 * tile + 1].astype(F32))
            gate_up[pl.ds(base, pad), at] = low[:pad].astype(BF16)
            gate_up[pl.ds(2 * pad + base, pad), at] = high[:pad].astype(BF16)
            down[pl.ds(base, half), at] = low[pad:].astype(BF16)
            down[pl.ds(base + half, half), at] = high[pad:].astype(BF16)
    for k in range(ny):
        prev[pl.ds(k * nx * rows, nx * rows)] = firsts[k][...]
    for k in range(nx):
        cotangent[pl.ds(k * ny * rows, ny * rows)] = seconds[k][...]
    pre = dot(prev[...], gate_up[...], ((1,), (1,)))
    gate_prev, up_prev = pre[:, : 2 * pad], pre[:, 2 * pad :]
    grad_hidden = turned(dot(cotangent[...], down[...], ((1,), (1,))), nx, ny, rows)
    sig = jax.nn.sigmoid(gate_prev)
    silu = gate_prev * sig
    grad_gate = grad_hidden * up_prev * sig * (1.0 + gate_prev * (1.0 - sig))
    grad_up = grad_hidden * silu
    hidden_prev = turned(silu * up_prev, ny, nx, rows)
    grads[:, : 2 * pad] = turned(grad_gate, ny, nx, rows).astype(BF16)
    grads[:, 2 * pad :] = turned(grad_up, ny, nx, rows).astype(BF16)
    for k, (value, tokens) in enumerate(((grad_gate, prev), (grad_up, prev), (hidden_prev, cotangent))):
        term = dot(value.astype(BF16).T, tokens[...], ((1,), (0,)))
        kept[pl.ds(k * pad, pad)] = term[:pad]
        sent[pl.ds(k * pad, pad)] = term[pad:].astype(BF16)


def input_kernel(grads, gate_up, *outs):
    rows = outs[0].shape[0]
    for k, out in enumerate(outs):
        at = pl.ds(k * rows, rows)
        out[...] = dot(grads[at, :], gate_up[...], ((1,), (0,))).astype(BF16)


def sum_kernel(count, *refs):
    parts, outs = refs[:count], refs[count:]
    rows = outs[0].shape[0]
    total = parts[0][...].astype(F32)
    for part in parts[1:]:
        total = total + part[...].astype(F32)
    for k, out in enumerate(outs):
        out[...] = total[k * rows : (k + 1) * rows].astype(BF16)


def pair_kernel(pad, kept, received, out):
    half = pad // 2
    for tile in range(out.shape[0] // 2):
        at = pl.ds(tile * LANES, LANES)
        total = kept[:, at] + received[:, at].astype(F32)
        left = jnp.concatenate((total[:pad], total[2 * pad : 2 * pad + half]))
        right = jnp.concatenate((total[pad : 2 * pad], total[2 * pad + half :]))
        even, odd = exchange_lanes(left, right)
        out[2 * tile] = even.astype(BF16)
        out[2 * tile + 1] = odd.astype(BF16)


def update_kernel(ny, part, pad, factor, arrived, gate, up, down_t, new_gate, new_up, new_down_t):
    half = pad // 2
    shard = down_t.shape[0]
    tops, lows = [], []
    for y in range(ny):
        total = arrived[y].astype(F32)
        for z in range(1, arrived.shape[0] // ny):
            total = total + arrived[z * ny + y].astype(F32)
        tops.append(total[:part])
        low = total[pad:]
        lows.append(low)
        lows.append(pltpu.roll(low, LANES // 2, 1)[: part - half])
    both = jnp.concatenate(tops).T
    new_gate[...] = gate[...] + factor * both[:shard]
    new_up[...] = up[...] + factor * both[shard:]
    new_down_t[...] = down_t[...] + factor * jnp.concatenate(lows).T[:shard]


def hidden_kernel(ny, nx, rows, pad, gate_up, *refs):
    firsts, seconds = refs[:ny], refs[ny : ny + nx]
    mine, theirs, hidden, tokens = refs[ny + nx :]
    half = tokens.shape[1]
    for k in range(ny):
        tokens[pl.ds(k * nx * rows, nx * rows)] = firsts[k][...]
    pre = dot(tokens[...], gate_up[:, :half], ((1,), (1,)))
    for k in range(nx):
        tokens[pl.ds(k * ny * rows, ny * rows)] = seconds[k][...]
    pre = pre + turned(dot(tokens[...], gate_up[:, half:], ((1,), (1,))), nx, ny, rows)
    value = jax.nn.silu(pre[:, : 2 * pad]) * pre[:, 2 * pad :]
    blank = jnp.zeros((value.shape[0], LANES - pad), F32)
    mine[...] = jnp.concatenate((value[:, :pad], blank), axis=1).astype(BF16)
    theirs[...] = jnp.concatenate((value[:, pad:], blank), axis=1).astype(BF16)
    hidden[...] = value.astype(BF16)


def output_kernel(hidden, down, mine, partner, *outs):
    rows = outs[0].shape[0]
    width = down.shape[1]
    for k, out in enumerate(outs):
        at = pl.ds(k * rows, rows)
        out[:, :width] = dot(hidden[at, :], down[...], ((1,), (0,))).astype(BF16)
        out[:, width : width + LANES] = mine[at, :]
        out[:, width + LANES :] = partner[at, :]


def arrival_kernel(nx, rows, part, place, *refs):
    ny = len(refs) - nx - 3
    parts, outs = refs[:ny], refs[ny : ny + nx]
    saved, by_y, by_x = refs[ny + nx :]
    width = outs[0].shape[1]
    total = parts[0][:, :width].astype(F32)
    for piece in parts[1:]:
        total = total + piece[:, :width].astype(F32)
    for k, out in enumerate(outs):
        out[...] = total[k * rows : (k + 1) * rows].astype(BF16)
    x, y, core = place[0], place[1], place[2]
    for k in range(ny):
        by_y[k] = parts[k][:, width:].astype(F32)
    pieces = [by_y[lax.rem(y - s + ny, ny)] for s in range(ny)]
    here = jnp.concatenate([piece[:, :part] for piece in pieces], axis=1)
    there = jnp.concatenate([piece[:, LANES : LANES + part] for piece in pieces], axis=1)
    low = jnp.where(core == 0, here, there)
    high = jnp.where(core == 0, there, here)
    for k in range(nx):
        by_x[k, :rows] = low[k * rows : (k + 1) * rows]
        by_x[k, rows:] = high[k * rows : (k + 1) * rows]
    ordered = [by_x[lax.rem(s - x + nx, nx)] for s in range(nx)]
    saved[...] = jnp.concatenate(ordered).astype(BF16)


def layer(x_next, x_prev, grad_out, gate_w, up_w, down_w, acc_gate, acc_up, acc_down):
    rows, width = x_prev.shape
    nz, ny, nx, nc = (lax.axis_size(name) for name in ALL)
    group = ny * nx * rows
    factor = 1.0 / math.sqrt(rows * nz * ny * nx * nc)
    units = gate_w.shape[1]
    part = units // ny
    pad = -(-part // 32) * 32
    block = (nz * ny, pad + pad // 2, LANES)
    mid = width // 2
    token_ops = 2 * group * 2 * pad * width

    first, second, packed = whole(
        functools.partial(front_kernel, nz, part, pad),
        (like((rows, width + mid), BF16), like((rows, width + mid), BF16), like(block, BF16)),
        (x_next, x_prev, grad_out, gate_w, up_w, down_w.T),
    )

    own = spread(packed, FS)
    other = swapped(own)

    first = jnp.stack(around(first, "x")).reshape(nx * rows, width + mid)
    second = jnp.stack(around(second, "y")).reshape(ny * rows, width + mid)
    prevs = around(first[:, :width], "y")
    cotangents = around(second[:, :width], "x")
    nexts = around(first[:, width:], "y")
    nexts = nexts + around(second[:, width:], "x")

    kept, sent, gate_up, down, grads = whole(
        functools.partial(backward_kernel, ny, nx, rows, pad),
        (
            like((3 * pad, width), F32),
            like((3 * pad, width), BF16),
            like((4 * pad, width), BF16),
            like((2 * pad, width), BF16),
            like((group, 4 * pad), BF16),
        ),
        (own, other, *prevs, *cotangents),
        (pltpu.VMEM((group, width), BF16), pltpu.VMEM((group, width), BF16)),
        flops=6 * token_ops,
        grant=20,
    )
    received = swapped(sent)
    input_parts = whole(
        input_kernel,
        tuple(like((ny * rows, width), BF16) for _ in range(nx)),
        (grads, gate_up),
        flops=2 * token_ops,
    )
    paired = whole(functools.partial(pair_kernel, pad), like(block, BF16), (kept, received))
    arrived = spread(paired, FS)
    new_gate, new_up, new_down_t = whole(
        functools.partial(update_kernel, ny, part, pad, factor),
        (like(acc_gate.shape, F32), like(acc_up.shape, F32), like(acc_down.shape[::-1], F32)),
        (arrived, acc_gate, acc_up, acc_down.T),
    )

    arrivals = for_owner(input_parts, "x")
    by_x = whole(
        functools.partial(sum_kernel, nx),
        tuple(like((rows, width), BF16) for _ in range(ny)),
        arrivals,
    )
    grad_input = added(for_owner(by_x, "y"))

    mine, theirs, hidden = whole(
        functools.partial(hidden_kernel, ny, nx, rows, pad),
        (like((group, LANES), BF16), like((group, LANES), BF16), like((group, 2 * pad), BF16)),
        (gate_up, *nexts),
        (pltpu.VMEM((group, mid), BF16),),
        flops=2 * token_ops,
    )
    partner = swapped(theirs)
    out_parts = whole(
        output_kernel,
        tuple(like((nx * rows, width + 2 * LANES), BF16) for _ in range(ny)),
        (hidden, down, mine, partner),
        flops=token_ops,
    )
    arrivals = for_owner(out_parts, "y")
    place = jnp.stack([lax.axis_index(name) for name in ("x", "y", "c")]).astype(jnp.int32)
    *by_y, saved = whole(
        functools.partial(arrival_kernel, nx, rows, part),
        (
            *(like((rows, width), BF16) for _ in range(nx)),
            like((nx * nc * rows, units), BF16),
        ),
        (place, *arrivals),
        (
            pltpu.VMEM((ny, nx * rows, 2 * LANES), F32),
            pltpu.VMEM((nx, nc * rows, units), F32),
        ),
        scalars=1,
    )
    out_next = added(for_owner(by_y, "x"))
    return out_next, saved, grad_input, new_gate, new_up, new_down_t.T


def solution(mesh):
    split = Mesh(mesh.devices.reshape(8, 4, 4, 2), ALL)
    tokens = P(ALL, None)
    wide, tall = P(FS, TP), P(TP, FS)
    in_specs = (tokens, tokens, tokens, wide, wide, tall, wide, wide, tall)
    out_specs = (tokens, wide, tokens, wide, wide, tall)
    return jax.shard_map(layer, mesh=split, in_specs=in_specs, out_specs=out_specs, check_vma=False)
```

```python
import functools
import math

import jax
import jax.numpy as jnp
from jax import lax
from jax.experimental import pallas as pl
from jax.experimental.pallas import tpu as pltpu
from jax.sharding import Mesh
from jax.sharding import PartitionSpec as P


BF16 = jnp.bfloat16
F32 = jnp.float32
FS = ("z", "y")
TP = ("x", "c")
ALL = ("z", "y", "x", "c")


def spread(blocks, axis):
    return lax.all_to_all(blocks, axis, 0, 0, tiled=True)


def swapped(array):
    return lax.ppermute(array, "c", [(0, 1), (1, 0)])


def moved(array, axis, step):
    length = lax.axis_size(axis)
    return lax.ppermute(array, axis, [(i, (i + step) % length) for i in range(length)])


def around(array, axis):
    return [array] + [moved(array, axis, -step) for step in range(1, lax.axis_size(axis))]


def for_owner(blocks, axis):
    return [blocks[0]] + [moved(blocks[step], axis, step) for step in range(1, len(blocks))]


def added(parts):
    total = parts[0].astype(F32)
    for part in parts[1:]:
        total = total + part.astype(F32)
    return total.astype(BF16)


def dot(left, right, dims):
    return lax.dot_general(left, right, (dims, ((), ())), preferred_element_type=F32)


LANES = 128


def whole(kernel, out_shape, inputs, scratch=(), flops=0, grant=12, spaces=None, result=pltpu.VMEM):
    spec = pl.BlockSpec(memory_space=result)
    spaces = spaces or [pltpu.VMEM] * len(inputs)
    single = not isinstance(out_shape, tuple)
    return pl.pallas_call(
        kernel,
        out_shape=out_shape,
        in_specs=[pl.BlockSpec(memory_space=space) for space in spaces],
        out_specs=spec if single else tuple(spec for _ in out_shape),
        scratch_shapes=scratch,
        compiler_params=pltpu.CompilerParams(vmem_limit_bytes=int(grant * 2**20)),
        cost_estimate=pl.CostEstimate(flops=flops, bytes_accessed=0, transcendentals=0),
    )(*inputs)


def fetched(sources, target, sems, first=0):
    rows = target.shape[0] // len(sources)
    copies = [
        pltpu.make_async_copy(source, target.at[pl.ds(k * rows, rows)], sems.at[first + k])
        for k, source in enumerate(sources)
    ]
    for copy in copies:
        copy.start()
    return copies


def like(shape, kind):
    return jax.ShapeDtypeStruct(shape, kind)


def exchange_lanes(left, right):
    half = LANES // 2
    lane = lax.broadcasted_iota(jnp.int32, left.shape, 1)
    low = jnp.where(lane < half, left, pltpu.roll(right, half, 1))
    high = jnp.where(lane < half, pltpu.roll(left, half, 1), right)
    return low, high


def front_kernel(copies, part, pad, *refs):
    sources, (first, second, out), refs = refs[:6], refs[6:9], refs[9:]
    targets, sems = refs[:6], refs[6]
    moves = [pltpu.make_async_copy(*pair, sems.at[k]) for k, pair in enumerate(zip(sources, targets))]
    for move in moves:
        move.start()
    for move in moves:
        move.wait()
    x_next, x_prev, grad_out, gate, up, down_t = targets
    width = x_prev.shape[1]
    mid = width // 2
    first[:, :width] = x_prev[...]
    first[:, width:] = x_next[:, :mid]
    second[:, :width] = grad_out[...]
    second[:, width:] = x_next[:, mid:]
    shard, units = gate.shape
    both = jnp.concatenate((gate[...], up[...]), axis=0).astype(F32).T
    tall = jnp.concatenate((down_t[...], jnp.zeros_like(down_t))).astype(F32).T[:, :shard]
    half = pad // 2
    count = units // part
    for y in range(count):
        top = both[y * part : (y + 1) * part]
        piece = tall[y * part : (y + 1) * part]
        ahead, behind = piece[:half], piece[half:]
        behind = jnp.concatenate((behind, jnp.zeros((pad - part, shard), F32)))
        low = jnp.concatenate((ahead, behind), axis=1)
        block = jnp.concatenate((top, jnp.zeros((pad - part, LANES), F32), low)).astype(BF16)
        for z in range(copies):
            out[z * count + y] = block


def turned(array, outer, inner, rows):
    return jnp.concatenate(
        [
            array[(o * inner + i) * rows : (o * inner + i + 1) * rows]
            for i in range(inner)
            for o in range(outer)
        ]
    )


def unpack_kernel(pad, own, other, gate_up, down):
    half = pad // 2
    for base, packed in ((0, own), (pad, other)):
        for tile in range(packed.shape[0] // 2):
            at = pl.ds(tile * LANES, LANES)
            low, high = exchange_lanes(packed[2 * tile].astype(F32), packed[2 * tile + 1].astype(F32))
            gate_up[pl.ds(base, pad), at] = low[:pad].astype(BF16)
            gate_up[pl.ds(2 * pad + base, pad), at] = high[:pad].astype(BF16)
            down[pl.ds(base, half), at] = low[pad:].astype(BF16)
            down[pl.ds(base + half, half), at] = high[pad:].astype(BF16)


def backward_kernel(ny, nx, rows, pad, gate_up, down, prev, cotangent, kept, sent, grads):
    pre = dot(prev[...], gate_up[...], ((1,), (1,)))
    gate_prev, up_prev = pre[:, : 2 * pad], pre[:, 2 * pad :]
    grad_hidden = turned(dot(cotangent[...], down[...], ((1,), (1,))), nx, ny, rows)
    sig = jax.nn.sigmoid(gate_prev)
    silu = gate_prev * sig
    grad_gate = grad_hidden * up_prev * sig * (1.0 + gate_prev * (1.0 - sig))
    grad_up = grad_hidden * silu
    hidden_prev = turned(silu * up_prev, ny, nx, rows)
    grads[:, : 2 * pad] = turned(grad_gate, ny, nx, rows).astype(BF16)
    grads[:, 2 * pad :] = turned(grad_up, ny, nx, rows).astype(BF16)
    for k, (value, tokens) in enumerate(((grad_gate, prev), (grad_up, prev), (hidden_prev, cotangent))):
        term = dot(value.astype(BF16).T, tokens[...], ((1,), (0,)))
        kept[pl.ds(k * pad, pad)] = term[:pad]
        sent[pl.ds(k * pad, pad)] = term[pad:].astype(BF16)


def input_kernel(grads, gate_up, *outs):
    rows = outs[0].shape[0]
    for k, out in enumerate(outs):
        at = pl.ds(k * rows, rows)
        out[...] = dot(grads[at, :], gate_up[...], ((1,), (0,))).astype(BF16)


def sum_kernel(count, *refs):
    parts, outs = refs[:count], refs[count:]
    rows = outs[0].shape[0]
    total = parts[0][...].astype(F32)
    for part in parts[1:]:
        total = total + part[...].astype(F32)
    for k, out in enumerate(outs):
        out[...] = total[k * rows : (k + 1) * rows].astype(BF16)


def pair_kernel(pad, kept, received, out):
    half = pad // 2
    for tile in range(out.shape[0] // 2):
        at = pl.ds(tile * LANES, LANES)
        total = kept[:, at] + received[:, at].astype(F32)
        left = jnp.concatenate((total[:pad], total[2 * pad : 2 * pad + half]))
        right = jnp.concatenate((total[pad : 2 * pad], total[2 * pad + half :]))
        even, odd = exchange_lanes(left, right)
        out[2 * tile] = even.astype(BF16)
        out[2 * tile + 1] = odd.astype(BF16)


def update_kernel(ny, part, pad, factor, arrived, gate, up, down_t, new_gate, new_up, new_down_t):
    half = pad // 2
    shard = down_t.shape[0]
    tops, lows = [], []
    for y in range(ny):
        total = arrived[y].astype(F32)
        for z in range(1, arrived.shape[0] // ny):
            total = total + arrived[z * ny + y].astype(F32)
        tops.append(total[:part])
        low = total[pad:]
        lows.append(low)
        lows.append(pltpu.roll(low, LANES // 2, 1)[: part - half])
    both = jnp.concatenate(tops).T
    new_gate[...] = gate[...] + factor * both[:shard]
    new_up[...] = up[...] + factor * both[shard:]
    new_down_t[...] = down_t[...] + factor * jnp.concatenate(lows).T[:shard]


def hidden_kernel(ny, nx, rows, pad, gate_up, *refs):
    firsts, seconds = refs[:ny], refs[ny : ny + nx]
    mine, theirs, hidden, left, right, sems = refs[ny + nx :]
    half = left.shape[1]
    moves = fetched(firsts, left, sems) + fetched(seconds, right, sems, ny)
    for move in moves:
        move.wait()
    pre = dot(left[...], gate_up[:, :half], ((1,), (1,)))
    pre = pre + turned(dot(right[...], gate_up[:, half:], ((1,), (1,))), nx, ny, rows)
    value = jax.nn.silu(pre[:, : 2 * pad]) * pre[:, 2 * pad :]
    blank = jnp.zeros((value.shape[0], LANES - pad), F32)
    mine[...] = jnp.concatenate((value[:, :pad], blank), axis=1).astype(BF16)
    theirs[...] = jnp.concatenate((value[:, pad:], blank), axis=1).astype(BF16)
    hidden[...] = value.astype(BF16)


def output_kernel(hidden, down, mine, partner, *outs):
    rows = outs[0].shape[0]
    width = down.shape[1]
    for k, out in enumerate(outs):
        at = pl.ds(k * rows, rows)
        out[:, :width] = dot(hidden[at, :], down[...], ((1,), (0,))).astype(BF16)
        out[:, width : width + LANES] = mine[at, :]
        out[:, width + LANES :] = partner[at, :]


def arrival_kernel(nx, rows, part, place, *refs):
    ny = len(refs) - nx - 3
    parts, outs = refs[:ny], refs[ny : ny + nx]
    saved, by_y, by_x = refs[ny + nx :]
    width = outs[0].shape[1]
    total = parts[0][:, :width].astype(F32)
    for piece in parts[1:]:
        total = total + piece[:, :width].astype(F32)
    for k, out in enumerate(outs):
        out[...] = total[k * rows : (k + 1) * rows].astype(BF16)
    x, y, core = place[0], place[1], place[2]
    for k in range(ny):
        by_y[k] = parts[k][:, width:].astype(F32)
    pieces = [by_y[lax.rem(y - s + ny, ny)] for s in range(ny)]
    here = jnp.concatenate([piece[:, :part] for piece in pieces], axis=1)
    there = jnp.concatenate([piece[:, LANES : LANES + part] for piece in pieces], axis=1)
    low = jnp.where(core == 0, here, there)
    high = jnp.where(core == 0, there, here)
    for k in range(nx):
        by_x[k, :rows] = low[k * rows : (k + 1) * rows]
        by_x[k, rows:] = high[k * rows : (k + 1) * rows]
    ordered = [by_x[lax.rem(s - x + nx, nx)] for s in range(nx)]
    saved[...] = jnp.concatenate(ordered).astype(BF16)


def layer(x_next, x_prev, grad_out, gate_w, up_w, down_w, acc_gate, acc_up, acc_down):
    rows, width = x_prev.shape
    nz, ny, nx, nc = (lax.axis_size(name) for name in ALL)
    group = ny * nx * rows
    factor = 1.0 / math.sqrt(rows * nz * ny * nx * nc)
    units = gate_w.shape[1]
    part = units // ny
    pad = -(-part // 32) * 32
    block = (nz * ny, pad + pad // 2, LANES)
    mid = width // 2
    token_ops = 2 * group * 2 * pad * width

    first, second, packed = whole(
        functools.partial(front_kernel, nz, part, pad),
        (like((rows, width + mid), BF16), like((rows, width + mid), BF16), like(block, BF16)),
        (x_next, x_prev, grad_out, gate_w, up_w, down_w.T),
        (
            *(pltpu.VMEM((rows, width), BF16) for _ in range(3)),
            *(pltpu.VMEM((width // (nz * ny), units), BF16) for _ in range(3)),
            pltpu.SemaphoreType.DMA((6,)),
        ),
        grant=60,
        spaces=[pltpu.HBM] * 6,
        result=None,
    )

    own = spread(packed, FS)
    other = swapped(own)

    first = jnp.stack(around(first, "x")).reshape(nx * rows, width + mid)
    second = jnp.stack(around(second, "y")).reshape(ny * rows, width + mid)
    prevs = around(first[:, :width], "y")
    cotangents = around(second[:, :width], "x")
    nexts = around(first[:, width:], "y")
    nexts = nexts + around(second[:, width:], "x")

    gate_up, down = whole(
        functools.partial(unpack_kernel, pad),
        (like((4 * pad, width), BF16), like((2 * pad, width), BF16)),
        (own, other),
    )

    prev = jnp.concatenate(prevs)
    cotangent = jnp.concatenate(cotangents)
    kept, sent, grads = whole(
        functools.partial(backward_kernel, ny, nx, rows, pad),
        (like((3 * pad, width), F32), like((3 * pad, width), BF16), like((group, 4 * pad), BF16)),
        (gate_up, down, prev, cotangent),
        flops=6 * token_ops,
    )
    received = swapped(sent)
    input_parts = whole(
        input_kernel,
        tuple(like((ny * rows, width), BF16) for _ in range(nx)),
        (grads, gate_up),
        flops=2 * token_ops,
    )
    paired = whole(functools.partial(pair_kernel, pad), like(block, BF16), (kept, received))
    arrived = spread(paired, FS)
    new_gate, new_up, new_down_t = whole(
        functools.partial(update_kernel, ny, part, pad, factor),
        (like(acc_gate.shape, F32), like(acc_up.shape, F32), like(acc_down.shape[::-1], F32)),
        (arrived, acc_gate, acc_up, acc_down.T),
    )

    arrivals = for_owner(input_parts, "x")
    by_x = whole(
        functools.partial(sum_kernel, nx),
        tuple(like((rows, width), BF16) for _ in range(ny)),
        arrivals,
    )
    grad_input = added(for_owner(by_x, "y"))

    mine, theirs, hidden = whole(
        functools.partial(hidden_kernel, ny, nx, rows, pad),
        (like((group, LANES), BF16), like((group, LANES), BF16), like((group, 2 * pad), BF16)),
        (gate_up, *nexts),
        (
            pltpu.VMEM((group, mid), BF16),
            pltpu.VMEM((group, mid), BF16),
            pltpu.SemaphoreType.DMA((ny + nx,)),
        ),
        flops=2 * token_ops,
        spaces=[pltpu.VMEM] + [pltpu.HBM] * (ny + nx),
    )
    partner = swapped(theirs)
    out_parts = whole(
        output_kernel,
        tuple(like((nx * rows, width + 2 * LANES), BF16) for _ in range(ny)),
        (hidden, down, mine, partner),
        flops=token_ops,
    )
    arrivals = for_owner(out_parts, "y")
    place = jnp.stack([lax.axis_index(name) for name in ("x", "y", "c")]).astype(jnp.int32)
    *by_y, saved = whole(
        functools.partial(arrival_kernel, nx, rows, part),
        (
            *(like((rows, width), BF16) for _ in range(nx)),
            like((nx * nc * rows, units), BF16),
        ),
        (place, *arrivals),
        (
            pltpu.VMEM((ny, nx * rows, 2 * LANES), F32),
            pltpu.VMEM((nx, nc * rows, units), F32),
        ),
        spaces=[pltpu.SMEM] + [pltpu.VMEM] * ny,
    )
    out_next = added(for_owner(by_y, "x"))
    return out_next, saved, grad_input, new_gate, new_up, new_down_t.T


def solution(mesh):
    split = Mesh(mesh.devices.reshape(8, 4, 4, 2), ALL)
    tokens = P(ALL, None)
    wide, tall = P(FS, TP), P(TP, FS)
    in_specs = (tokens, tokens, tokens, wide, wide, tall, wide, wide, tall)
    out_specs = (tokens, wide, tokens, wide, wide, tall)
    return jax.shard_map(layer, mesh=split, in_specs=in_specs, out_specs=out_specs, check_vma=False)
```

```python
import functools
import math

import jax
import jax.numpy as jnp
from jax import lax
from jax.experimental import pallas as pl
from jax.experimental.pallas import tpu as pltpu
from jax.sharding import Mesh
from jax.sharding import PartitionSpec as P


BF16 = jnp.bfloat16
F32 = jnp.float32
FS = ("z", "y")
TP = ("x", "c")
ALL = ("z", "y", "x", "c")


def spread(blocks, axis):
    return lax.all_to_all(blocks, axis, 0, 0, tiled=True)


def swapped(array):
    return lax.ppermute(array, "c", [(0, 1), (1, 0)])


def moved(array, axis, step):
    length = lax.axis_size(axis)
    return lax.ppermute(array, axis, [(i, (i + step) % length) for i in range(length)])


def around(array, axis):
    return [array] + [moved(array, axis, -step) for step in range(1, lax.axis_size(axis))]


def for_owner(blocks, axis):
    return [blocks[0]] + [moved(blocks[step], axis, step) for step in range(1, len(blocks))]


def added(parts):
    total = parts[0].astype(F32)
    for part in parts[1:]:
        total = total + part.astype(F32)
    return total.astype(BF16)


def dot(left, right, dims):
    return lax.dot_general(left, right, (dims, ((), ())), preferred_element_type=F32)


LANES = 128


def whole(kernel, out_shape, inputs, scratch=(), flops=0, grant=12, spaces=None, result=pltpu.VMEM):
    spec = pl.BlockSpec(memory_space=result)
    spaces = spaces or [pltpu.VMEM] * len(inputs)
    single = not isinstance(out_shape, tuple)
    return pl.pallas_call(
        kernel,
        out_shape=out_shape,
        in_specs=[pl.BlockSpec(memory_space=space) for space in spaces],
        out_specs=spec if single else tuple(spec for _ in out_shape),
        scratch_shapes=scratch,
        compiler_params=pltpu.CompilerParams(vmem_limit_bytes=int(grant * 2**20)),
        cost_estimate=pl.CostEstimate(flops=flops, bytes_accessed=0, transcendentals=0),
    )(*inputs)


def fetched(sources, target, sems):
    rows = target.shape[0] // len(sources)
    copies = [
        pltpu.make_async_copy(source, target.at[pl.ds(k * rows, rows)], sems.at[k])
        for k, source in enumerate(sources)
    ]
    for copy in copies:
        copy.start()
    return copies


def like(shape, kind):
    return jax.ShapeDtypeStruct(shape, kind)


def exchange_lanes(left, right):
    half = LANES // 2
    lane = lax.broadcasted_iota(jnp.int32, left.shape, 1)
    low = jnp.where(lane < half, left, pltpu.roll(right, half, 1))
    high = jnp.where(lane < half, pltpu.roll(left, half, 1), right)
    return low, high


def front_kernel(copies, part, pad, *refs):
    sources, (second, out), refs = refs[:5], refs[5:7], refs[7:]
    targets, sems = refs[:5], refs[5]
    moves = [pltpu.make_async_copy(*pair, sems.at[k]) for k, pair in enumerate(zip(sources, targets))]
    for move in moves:
        move.start()
    for move in moves:
        move.wait()
    x_next, grad_out, gate, up, down_t = targets
    width = grad_out.shape[1]
    second[:, :width] = grad_out[...]
    second[:, width:] = x_next[...]
    shard, units = gate.shape
    both = jnp.concatenate((gate[...], up[...]), axis=0).astype(F32).T
    tall = jnp.concatenate((down_t[...], jnp.zeros_like(down_t))).astype(F32).T[:, :shard]
    half = pad // 2
    count = units // part
    for y in range(count):
        top = both[y * part : (y + 1) * part]
        piece = tall[y * part : (y + 1) * part]
        ahead, behind = piece[:half], piece[half:]
        behind = jnp.concatenate((behind, jnp.zeros((pad - part, shard), F32)))
        low = jnp.concatenate((ahead, behind), axis=1)
        block = jnp.concatenate((top, jnp.zeros((pad - part, LANES), F32), low)).astype(BF16)
        for z in range(copies):
            out[z * count + y] = block


def turned(array, outer, inner, rows):
    return jnp.concatenate(
        [
            array[(o * inner + i) * rows : (o * inner + i + 1) * rows]
            for i in range(inner)
            for o in range(outer)
        ]
    )


def unpack_kernel(pad, own, other, gate_up, down):
    half = pad // 2
    for base, packed in ((0, own), (pad, other)):
        for tile in range(packed.shape[0] // 2):
            at = pl.ds(tile * LANES, LANES)
            low, high = exchange_lanes(packed[2 * tile].astype(F32), packed[2 * tile + 1].astype(F32))
            gate_up[pl.ds(base, pad), at] = low[:pad].astype(BF16)
            gate_up[pl.ds(2 * pad + base, pad), at] = high[:pad].astype(BF16)
            down[pl.ds(base, half), at] = low[pad:].astype(BF16)
            down[pl.ds(base + half, half), at] = high[pad:].astype(BF16)


def backward_kernel(ny, nx, rows, pad, gate_up, down, prev, cotangent, kept, sent, grads):
    pre = dot(prev[...], gate_up[...], ((1,), (1,)))
    gate_prev, up_prev = pre[:, : 2 * pad], pre[:, 2 * pad :]
    grad_hidden = turned(dot(cotangent[...], down[...], ((1,), (1,))), nx, ny, rows)
    sig = jax.nn.sigmoid(gate_prev)
    silu = gate_prev * sig
    grad_gate = grad_hidden * up_prev * sig * (1.0 + gate_prev * (1.0 - sig))
    grad_up = grad_hidden * silu
    hidden_prev = turned(silu * up_prev, ny, nx, rows)
    grads[:, : 2 * pad] = turned(grad_gate, ny, nx, rows).astype(BF16)
    grads[:, 2 * pad :] = turned(grad_up, ny, nx, rows).astype(BF16)
    for k, (value, tokens) in enumerate(((grad_gate, prev), (grad_up, prev), (hidden_prev, cotangent))):
        term = dot(value.astype(BF16).T, tokens[...], ((1,), (0,)))
        kept[pl.ds(k * pad, pad)] = term[:pad]
        sent[pl.ds(k * pad, pad)] = term[pad:].astype(BF16)


def input_kernel(grads, gate_up, *outs):
    rows = outs[0].shape[0]
    for k, out in enumerate(outs):
        at = pl.ds(k * rows, rows)
        out[...] = dot(grads[at, :], gate_up[...], ((1,), (0,))).astype(BF16)


def sum_kernel(count, *refs):
    parts, outs = refs[:count], refs[count:]
    rows = outs[0].shape[0]
    total = parts[0][...].astype(F32)
    for part in parts[1:]:
        total = total + part[...].astype(F32)
    for k, out in enumerate(outs):
        out[...] = total[k * rows : (k + 1) * rows].astype(BF16)


def pair_kernel(pad, kept, received, out):
    half = pad // 2
    for tile in range(out.shape[0] // 2):
        at = pl.ds(tile * LANES, LANES)
        total = kept[:, at] + received[:, at].astype(F32)
        left = jnp.concatenate((total[:pad], total[2 * pad : 2 * pad + half]))
        right = jnp.concatenate((total[pad : 2 * pad], total[2 * pad + half :]))
        even, odd = exchange_lanes(left, right)
        out[2 * tile] = even.astype(BF16)
        out[2 * tile + 1] = odd.astype(BF16)


def update_kernel(ny, part, pad, factor, arrived, gate, up, down_t, new_gate, new_up, new_down_t):
    half = pad // 2
    shard = down_t.shape[0]
    tops, lows = [], []
    for y in range(ny):
        total = arrived[y].astype(F32)
        for z in range(1, arrived.shape[0] // ny):
            total = total + arrived[z * ny + y].astype(F32)
        tops.append(total[:part])
        low = total[pad:]
        lows.append(low)
        lows.append(pltpu.roll(low, LANES // 2, 1)[: part - half])
    both = jnp.concatenate(tops).T
    new_gate[...] = gate[...] + factor * both[:shard]
    new_up[...] = up[...] + factor * both[shard:]
    new_down_t[...] = down_t[...] + factor * jnp.concatenate(lows).T[:shard]


def hidden_kernel(ny, nx, rows, pad, gate_up, *refs):
    pieces, (mine, theirs, hidden, tokens, sems) = refs[:nx], refs[nx:]
    for move in fetched(pieces, tokens, sems):
        move.wait()
    pre = turned(dot(tokens[...], gate_up[...], ((1,), (1,))), nx, ny, rows)
    value = jax.nn.silu(pre[:, : 2 * pad]) * pre[:, 2 * pad :]
    blank = jnp.zeros((value.shape[0], LANES - pad), F32)
    mine[...] = jnp.concatenate((value[:, :pad], blank), axis=1).astype(BF16)
    theirs[...] = jnp.concatenate((value[:, pad:], blank), axis=1).astype(BF16)
    hidden[...] = value.astype(BF16)


def output_kernel(hidden, down, mine, partner, *outs):
    rows = outs[0].shape[0]
    width = down.shape[1]
    for k, out in enumerate(outs):
        at = pl.ds(k * rows, rows)
        out[:, :width] = dot(hidden[at, :], down[...], ((1,), (0,))).astype(BF16)
        out[:, width : width + LANES] = mine[at, :]
        out[:, width + LANES :] = partner[at, :]


def arrival_kernel(nx, rows, part, place, *refs):
    ny = len(refs) - nx - 3
    parts, outs = refs[:ny], refs[ny : ny + nx]
    saved, by_y, by_x = refs[ny + nx :]
    width = outs[0].shape[1]
    total = parts[0][:, :width].astype(F32)
    for piece in parts[1:]:
        total = total + piece[:, :width].astype(F32)
    for k, out in enumerate(outs):
        out[...] = total[k * rows : (k + 1) * rows].astype(BF16)
    x, y, core = place[0], place[1], place[2]
    for k in range(ny):
        by_y[k] = parts[k][:, width:].astype(F32)
    pieces = [by_y[lax.rem(y - s + ny, ny)] for s in range(ny)]
    here = jnp.concatenate([piece[:, :part] for piece in pieces], axis=1)
    there = jnp.concatenate([piece[:, LANES : LANES + part] for piece in pieces], axis=1)
    low = jnp.where(core == 0, here, there)
    high = jnp.where(core == 0, there, here)
    for k in range(nx):
        by_x[k, :rows] = low[k * rows : (k + 1) * rows]
        by_x[k, rows:] = high[k * rows : (k + 1) * rows]
    ordered = [by_x[lax.rem(s - x + nx, nx)] for s in range(nx)]
    saved[...] = jnp.concatenate(ordered).astype(BF16)


def layer(x_next, x_prev, grad_out, gate_w, up_w, down_w, acc_gate, acc_up, acc_down):
    rows, width = x_prev.shape
    nz, ny, nx, nc = (lax.axis_size(name) for name in ALL)
    group = ny * nx * rows
    factor = 1.0 / math.sqrt(rows * nz * ny * nx * nc)
    units = gate_w.shape[1]
    part = units // ny
    pad = -(-part // 32) * 32
    block = (nz * ny, pad + pad // 2, LANES)
    token_ops = 2 * group * 2 * pad * width

    second, packed = whole(
        functools.partial(front_kernel, nz, part, pad),
        (like((rows, 2 * width), BF16), like(block, BF16)),
        (x_next, grad_out, gate_w, up_w, down_w.T),
        (
            *(pltpu.VMEM((rows, width), BF16) for _ in range(2)),
            *(pltpu.VMEM((width // (nz * ny), units), BF16) for _ in range(3)),
            pltpu.SemaphoreType.DMA((5,)),
        ),
        grant=60,
        spaces=[pltpu.HBM] * 5,
        result=None,
    )

    own = spread(packed, FS)
    other = swapped(own)

    first = jnp.stack(around(x_prev, "x")).reshape(nx * rows, width)
    second = jnp.stack(around(second, "y")).reshape(ny * rows, 2 * width)
    prevs = around(first, "y")
    cotangents = around(second[:, :width], "x")
    nexts = around(second[:, width:], "x")
    gate_up, down = whole(
        functools.partial(unpack_kernel, pad),
        (like((4 * pad, width), BF16), like((2 * pad, width), BF16)),
        (own, other),
    )

    prev = jnp.concatenate(prevs)
    cotangent = jnp.concatenate(cotangents)
    kept, sent, grads = whole(
        functools.partial(backward_kernel, ny, nx, rows, pad),
        (like((3 * pad, width), F32), like((3 * pad, width), BF16), like((group, 4 * pad), BF16)),
        (gate_up, down, prev, cotangent),
        flops=6 * token_ops,
    )
    received = swapped(sent)
    input_parts = whole(
        input_kernel,
        tuple(like((ny * rows, width), BF16) for _ in range(nx)),
        (grads, gate_up),
        flops=2 * token_ops,
    )
    paired = whole(functools.partial(pair_kernel, pad), like(block, BF16), (kept, received))
    arrived = spread(paired, FS)
    new_gate, new_up, new_down_t = whole(
        functools.partial(update_kernel, ny, part, pad, factor),
        (like(acc_gate.shape, F32), like(acc_up.shape, F32), like(acc_down.shape[::-1], F32)),
        (arrived, acc_gate, acc_up, acc_down.T),
    )

    arrivals = for_owner(input_parts, "x")
    by_x = whole(
        functools.partial(sum_kernel, nx),
        tuple(like((rows, width), BF16) for _ in range(ny)),
        arrivals,
    )
    grad_input = added(for_owner(by_x, "y"))

    mine, theirs, hidden = whole(
        functools.partial(hidden_kernel, ny, nx, rows, pad),
        (like((group, LANES), BF16), like((group, LANES), BF16), like((group, 2 * pad), BF16)),
        (gate_up, *nexts),
        (pltpu.VMEM((group, width), BF16), pltpu.SemaphoreType.DMA((nx,))),
        flops=2 * token_ops,
        spaces=[pltpu.VMEM] + [pltpu.HBM] * nx,
    )
    partner = swapped(theirs)
    out_parts = whole(
        output_kernel,
        tuple(like((nx * rows, width + 2 * LANES), BF16) for _ in range(ny)),
        (hidden, down, mine, partner),
        flops=token_ops,
    )
    arrivals = for_owner(out_parts, "y")
    place = jnp.stack([lax.axis_index(name) for name in ("x", "y", "c")]).astype(jnp.int32)
    *by_y, saved = whole(
        functools.partial(arrival_kernel, nx, rows, part),
        (
            *(like((rows, width), BF16) for _ in range(nx)),
            like((nx * nc * rows, units), BF16),
        ),
        (place, *arrivals),
        (
            pltpu.VMEM((ny, nx * rows, 2 * LANES), F32),
            pltpu.VMEM((nx, nc * rows, units), F32),
        ),
        spaces=[pltpu.SMEM] + [pltpu.VMEM] * ny,
    )
    out_next = added(for_owner(by_y, "x"))
    return out_next, saved, grad_input, new_gate, new_up, new_down_t.T


def solution(mesh):
    split = Mesh(mesh.devices.reshape(8, 4, 4, 2), ALL)
    tokens = P(ALL, None)
    wide, tall = P(FS, TP), P(TP, FS)
    in_specs = (tokens, tokens, tokens, wide, wide, tall, wide, wide, tall)
    out_specs = (tokens, wide, tokens, wide, wide, tall)
    return jax.shard_map(layer, mesh=split, in_specs=in_specs, out_specs=out_specs, check_vma=False)
```

```python
import functools
import math

import jax
import jax.numpy as jnp
from jax import lax
from jax.experimental import pallas as pl
from jax.experimental.pallas import tpu as pltpu
from jax.sharding import Mesh
from jax.sharding import PartitionSpec as P


BF16 = jnp.bfloat16
F32 = jnp.float32
FS = ("z", "y")
TP = ("x", "c")
ALL = ("z", "y", "x", "c")


def spread(blocks, axis):
    return lax.all_to_all(blocks, axis, 0, 0, tiled=True)


def swapped(array):
    return lax.ppermute(array, "c", [(0, 1), (1, 0)])


def moved(array, axis, step):
    length = lax.axis_size(axis)
    return lax.ppermute(array, axis, [(i, (i + step) % length) for i in range(length)])


def around(array, axis):
    return [array] + [moved(array, axis, -step) for step in range(1, lax.axis_size(axis))]


def for_owner(blocks, axis):
    return [blocks[0]] + [moved(blocks[step], axis, step) for step in range(1, len(blocks))]


def added(parts):
    total = parts[0].astype(F32)
    for part in parts[1:]:
        total = total + part.astype(F32)
    return total.astype(BF16)


def dot(left, right, dims):
    return lax.dot_general(left, right, (dims, ((), ())), preferred_element_type=F32)


LANES = 128


def whole(kernel, out_shape, inputs, scratch=(), flops=0, grant=12, spaces=None, result=pltpu.VMEM):
    spec = pl.BlockSpec(memory_space=result)
    spaces = spaces or [pltpu.VMEM] * len(inputs)
    single = not isinstance(out_shape, tuple)
    return pl.pallas_call(
        kernel,
        out_shape=out_shape,
        in_specs=[pl.BlockSpec(memory_space=space) for space in spaces],
        out_specs=spec if single else tuple(spec for _ in out_shape),
        scratch_shapes=scratch,
        compiler_params=pltpu.CompilerParams(vmem_limit_bytes=int(grant * 2**20)),
        cost_estimate=pl.CostEstimate(flops=flops, bytes_accessed=0, transcendentals=0),
    )(*inputs)


def fetched(sources, target, sems):
    rows = target.shape[0] // len(sources)
    copies = [
        pltpu.make_async_copy(source, target.at[pl.ds(k * rows, rows)], sems.at[k])
        for k, source in enumerate(sources)
    ]
    for copy in copies:
        copy.start()
    return copies


def like(shape, kind):
    return jax.ShapeDtypeStruct(shape, kind)


def exchange_lanes(left, right):
    half = LANES // 2
    lane = lax.broadcasted_iota(jnp.int32, left.shape, 1)
    low = jnp.where(lane < half, left, pltpu.roll(right, half, 1))
    high = jnp.where(lane < half, pltpu.roll(left, half, 1), right)
    return low, high


def front_kernel(copies, part, pad, *refs):
    sources, (second, out), refs = refs[:5], refs[5:7], refs[7:]
    targets, sems = refs[:5], refs[5]
    moves = [pltpu.make_async_copy(*pair, sems.at[k]) for k, pair in enumerate(zip(sources, targets))]
    for move in moves:
        move.start()
    for move in moves:
        move.wait()
    x_next, grad_out, gate, up, down_t = targets
    width = grad_out.shape[1]
    second[:, :width] = grad_out[...]
    second[:, width:] = x_next[...]
    shard, units = gate.shape
    both = jnp.concatenate((gate[...], up[...]), axis=0).astype(F32).T
    tall = jnp.concatenate((down_t[...], jnp.zeros_like(down_t))).astype(F32).T[:, :shard]
    half = pad // 2
    count = units // part
    for y in range(count):
        top = both[y * part : (y + 1) * part]
        piece = tall[y * part : (y + 1) * part]
        ahead, behind = piece[:half], piece[half:]
        behind = jnp.concatenate((behind, jnp.zeros((pad - part, shard), F32)))
        low = jnp.concatenate((ahead, behind), axis=1)
        block = jnp.concatenate((top, low)).astype(BF16)
        for z in range(copies):
            out[z * count + y] = block


def turned(array, outer, inner, rows):
    return jnp.concatenate(
        [
            array[(o * inner + i) * rows : (o * inner + i + 1) * rows]
            for i in range(inner)
            for o in range(outer)
        ]
    )


def unpack_kernel(part, pad, own, other, gate_up, down):
    half = pad // 2
    blank = jnp.zeros((pad - part, LANES), F32)
    for base, packed in ((0, own), (pad, other)):
        for tile in range(packed.shape[0] // 2):
            at = pl.ds(tile * LANES, LANES)
            low, high = exchange_lanes(packed[2 * tile].astype(F32), packed[2 * tile + 1].astype(F32))
            for row, value in ((base, low), (2 * pad + base, high)):
                gate_up[pl.ds(row, pad), at] = jnp.concatenate((value[:part], blank)).astype(BF16)
            down[pl.ds(base, half), at] = low[part:].astype(BF16)
            down[pl.ds(base + half, half), at] = high[part:].astype(BF16)


def backward_kernel(ny, nx, rows, pad, gate_up, down, prev, cotangent, kept, sent, grads):
    pre = dot(prev[...], gate_up[...], ((1,), (1,)))
    gate_prev, up_prev = pre[:, : 2 * pad], pre[:, 2 * pad :]
    grad_hidden = turned(dot(cotangent[...], down[...], ((1,), (1,))), nx, ny, rows)
    sig = jax.nn.sigmoid(gate_prev)
    silu = gate_prev * sig
    grad_gate = grad_hidden * up_prev * sig * (1.0 + gate_prev * (1.0 - sig))
    grad_up = grad_hidden * silu
    hidden_prev = turned(silu * up_prev, ny, nx, rows)
    grads[:, : 2 * pad] = turned(grad_gate, ny, nx, rows).astype(BF16)
    grads[:, 2 * pad :] = turned(grad_up, ny, nx, rows).astype(BF16)
    for k, (value, tokens) in enumerate(((grad_gate, prev), (grad_up, prev), (hidden_prev, cotangent))):
        term = dot(value.astype(BF16).T, tokens[...], ((1,), (0,)))
        kept[pl.ds(k * pad, pad)] = term[:pad]
        sent[pl.ds(k * pad, pad)] = term[pad:].astype(BF16)


def input_kernel(grads, gate_up, *outs):
    rows = outs[0].shape[0]
    for k, out in enumerate(outs):
        at = pl.ds(k * rows, rows)
        out[...] = dot(grads[at, :], gate_up[...], ((1,), (0,))).astype(BF16)


def sum_kernel(count, *refs):
    parts, outs = refs[:count], refs[count:]
    rows = outs[0].shape[0]
    total = parts[0][...].astype(F32)
    for part in parts[1:]:
        total = total + part[...].astype(F32)
    for k, out in enumerate(outs):
        out[...] = total[k * rows : (k + 1) * rows].astype(BF16)


def pair_kernel(part, pad, kept, received, out):
    half = pad // 2
    for tile in range(out.shape[0] // 2):
        at = pl.ds(tile * LANES, LANES)
        total = kept[:, at] + received[:, at].astype(F32)
        left = jnp.concatenate((total[:part], total[2 * pad : 2 * pad + half]))
        right = jnp.concatenate((total[pad : pad + part], total[2 * pad + half :]))
        even, odd = exchange_lanes(left, right)
        out[2 * tile] = even.astype(BF16)
        out[2 * tile + 1] = odd.astype(BF16)


def update_kernel(ny, part, pad, factor, arrived, gate, up, down_t, new_gate, new_up, new_down_t):
    half = pad // 2
    shard = down_t.shape[0]
    tops, lows = [], []
    for y in range(ny):
        total = arrived[y].astype(F32)
        for z in range(1, arrived.shape[0] // ny):
            total = total + arrived[z * ny + y].astype(F32)
        tops.append(total[:part])
        low = total[part:]
        lows.append(low)
        lows.append(pltpu.roll(low, LANES // 2, 1)[: part - half])
    both = jnp.concatenate(tops).T
    new_gate[...] = gate[...] + factor * both[:shard]
    new_up[...] = up[...] + factor * both[shard:]
    new_down_t[...] = down_t[...] + factor * jnp.concatenate(lows).T[:shard]


def hidden_kernel(ny, nx, rows, pad, gate_up, *refs):
    pieces, (mine, theirs, hidden, tokens, sems) = refs[:nx], refs[nx:]
    for move in fetched(pieces, tokens, sems):
        move.wait()
    pre = turned(dot(tokens[...], gate_up[...], ((1,), (1,))), nx, ny, rows)
    value = jax.nn.silu(pre[:, : 2 * pad]) * pre[:, 2 * pad :]
    blank = jnp.zeros((value.shape[0], LANES - pad), F32)
    mine[...] = jnp.concatenate((value[:, :pad], blank), axis=1).astype(BF16)
    theirs[...] = jnp.concatenate((value[:, pad:], blank), axis=1).astype(BF16)
    hidden[...] = value.astype(BF16)


def output_kernel(hidden, down, mine, partner, *outs):
    rows = outs[0].shape[0]
    width = down.shape[1]
    for k, out in enumerate(outs):
        at = pl.ds(k * rows, rows)
        out[:, :width] = dot(hidden[at, :], down[...], ((1,), (0,))).astype(BF16)
        out[:, width : width + LANES] = mine[at, :]
        out[:, width + LANES :] = partner[at, :]


def arrival_kernel(nx, rows, part, place, *refs):
    ny = len(refs) - nx - 3
    parts, outs = refs[:ny], refs[ny : ny + nx]
    saved, by_y, by_x = refs[ny + nx :]
    width = outs[0].shape[1]
    total = parts[0][:, :width].astype(F32)
    for piece in parts[1:]:
        total = total + piece[:, :width].astype(F32)
    for k, out in enumerate(outs):
        out[...] = total[k * rows : (k + 1) * rows].astype(BF16)
    x, y, core = place[0], place[1], place[2]
    for k in range(ny):
        by_y[k] = parts[k][:, width:].astype(F32)
    pieces = [by_y[lax.rem(y - s + ny, ny)] for s in range(ny)]
    here = jnp.concatenate([piece[:, :part] for piece in pieces], axis=1)
    there = jnp.concatenate([piece[:, LANES : LANES + part] for piece in pieces], axis=1)
    low = jnp.where(core == 0, here, there)
    high = jnp.where(core == 0, there, here)
    for k in range(nx):
        by_x[k, :rows] = low[k * rows : (k + 1) * rows]
        by_x[k, rows:] = high[k * rows : (k + 1) * rows]
    ordered = [by_x[lax.rem(s - x + nx, nx)] for s in range(nx)]
    saved[...] = jnp.concatenate(ordered).astype(BF16)


def layer(x_next, x_prev, grad_out, gate_w, up_w, down_w, acc_gate, acc_up, acc_down):
    rows, width = x_prev.shape
    nz, ny, nx, nc = (lax.axis_size(name) for name in ALL)
    group = ny * nx * rows
    factor = 1.0 / math.sqrt(rows * nz * ny * nx * nc)
    units = gate_w.shape[1]
    part = units // ny
    pad = -(-part // 32) * 32
    block = (nz * ny, part + pad // 2, LANES)
    token_ops = 2 * group * 2 * pad * width

    second, packed = whole(
        functools.partial(front_kernel, nz, part, pad),
        (like((rows, 2 * width), BF16), like(block, BF16)),
        (x_next, grad_out, gate_w, up_w, down_w.T),
        (
            *(pltpu.VMEM((rows, width), BF16) for _ in range(2)),
            *(pltpu.VMEM((width // (nz * ny), units), BF16) for _ in range(3)),
            pltpu.SemaphoreType.DMA((5,)),
        ),
        grant=60,
        spaces=[pltpu.HBM] * 5,
        result=None,
    )

    own = spread(packed, FS)
    other = swapped(own)

    first = jnp.stack(around(x_prev, "x")).reshape(nx * rows, width)
    second = jnp.stack(around(second, "y")).reshape(ny * rows, 2 * width)
    prevs = around(first, "y")
    cotangents = around(second[:, :width], "x")
    nexts = around(second[:, width:], "x")
    gate_up, down = whole(
        functools.partial(unpack_kernel, part, pad),
        (like((4 * pad, width), BF16), like((2 * pad, width), BF16)),
        (own, other),
    )

    prev = jnp.concatenate(prevs)
    cotangent = jnp.concatenate(cotangents)
    kept, sent, grads = whole(
        functools.partial(backward_kernel, ny, nx, rows, pad),
        (like((3 * pad, width), F32), like((3 * pad, width), BF16), like((group, 4 * pad), BF16)),
        (gate_up, down, prev, cotangent),
        flops=6 * token_ops,
    )
    received = swapped(sent)
    input_parts = whole(
        input_kernel,
        tuple(like((ny * rows, width), BF16) for _ in range(nx)),
        (grads, gate_up),
        flops=2 * token_ops,
    )
    paired = whole(functools.partial(pair_kernel, part, pad), like(block, BF16), (kept, received))
    arrived = spread(paired, FS)
    new_gate, new_up, new_down_t = whole(
        functools.partial(update_kernel, ny, part, pad, factor),
        (like(acc_gate.shape, F32), like(acc_up.shape, F32), like(acc_down.shape[::-1], F32)),
        (arrived, acc_gate, acc_up, acc_down.T),
    )

    arrivals = for_owner(input_parts, "x")
    by_x = whole(
        functools.partial(sum_kernel, nx),
        tuple(like((rows, width), BF16) for _ in range(ny)),
        arrivals,
    )
    grad_input = added(for_owner(by_x, "y"))

    mine, theirs, hidden = whole(
        functools.partial(hidden_kernel, ny, nx, rows, pad),
        (like((group, LANES), BF16), like((group, LANES), BF16), like((group, 2 * pad), BF16)),
        (gate_up, *nexts),
        (pltpu.VMEM((group, width), BF16), pltpu.SemaphoreType.DMA((nx,))),
        flops=2 * token_ops,
        spaces=[pltpu.VMEM] + [pltpu.HBM] * nx,
    )
    partner = swapped(theirs)
    out_parts = whole(
        output_kernel,
        tuple(like((nx * rows, width + 2 * LANES), BF16) for _ in range(ny)),
        (hidden, down, mine, partner),
        flops=token_ops,
    )
    arrivals = for_owner(out_parts, "y")
    place = jnp.stack([lax.axis_index(name) for name in ("x", "y", "c")]).astype(jnp.int32)
    *by_y, saved = whole(
        functools.partial(arrival_kernel, nx, rows, part),
        (
            *(like((rows, width), BF16) for _ in range(nx)),
            like((nx * nc * rows, units), BF16),
        ),
        (place, *arrivals),
        (
            pltpu.VMEM((ny, nx * rows, 2 * LANES), F32),
            pltpu.VMEM((nx, nc * rows, units), F32),
        ),
        spaces=[pltpu.SMEM] + [pltpu.VMEM] * ny,
    )
    out_next = added(for_owner(by_y, "x"))
    return out_next, saved, grad_input, new_gate, new_up, new_down_t.T


def solution(mesh):
    split = Mesh(mesh.devices.reshape(8, 4, 4, 2), ALL)
    tokens = P(ALL, None)
    wide, tall = P(FS, TP), P(TP, FS)
    in_specs = (tokens, tokens, tokens, wide, wide, tall, wide, wide, tall)
    out_specs = (tokens, wide, tokens, wide, wide, tall)
    return jax.shard_map(layer, mesh=split, in_specs=in_specs, out_specs=out_specs, check_vma=False)
```

```python
import functools
import math

import jax
import jax.numpy as jnp
from jax import lax
from jax.experimental import pallas as pl
from jax.experimental.pallas import tpu as pltpu
from jax.sharding import Mesh
from jax.sharding import PartitionSpec as P


BF16 = jnp.bfloat16
F32 = jnp.float32
FS = ("z", "y")
TP = ("x", "c")
ALL = ("z", "y", "x", "c")


def spread(blocks, axis):
    return lax.all_to_all(blocks, axis, 0, 0, tiled=True)


def swapped(array):
    return lax.ppermute(array, "c", [(0, 1), (1, 0)])


def moved(array, axis, step):
    length = lax.axis_size(axis)
    return lax.ppermute(array, axis, [(i, (i + step) % length) for i in range(length)])


def around(array, axis):
    return [array] + [moved(array, axis, -step) for step in range(1, lax.axis_size(axis))]


def for_owner(blocks, axis):
    return [blocks[0]] + [moved(blocks[step], axis, step) for step in range(1, len(blocks))]


def added(parts):
    total = parts[0].astype(F32)
    for part in parts[1:]:
        total = total + part.astype(F32)
    return total.astype(BF16)


def dot(left, right, dims):
    return lax.dot_general(left, right, (dims, ((), ())), preferred_element_type=F32)


LANES = 128


def whole(kernel, out_shape, inputs, scratch=(), flops=0, grant=12, spaces=None, result=pltpu.VMEM):
    spec = pl.BlockSpec(memory_space=result)
    spaces = spaces or [pltpu.VMEM] * len(inputs)
    single = not isinstance(out_shape, tuple)
    return pl.pallas_call(
        kernel,
        out_shape=out_shape,
        in_specs=[pl.BlockSpec(memory_space=space) for space in spaces],
        out_specs=spec if single else tuple(spec for _ in out_shape),
        scratch_shapes=scratch,
        compiler_params=pltpu.CompilerParams(vmem_limit_bytes=int(grant * 2**20)),
        cost_estimate=pl.CostEstimate(flops=flops, bytes_accessed=0, transcendentals=0),
    )(*inputs)


def fetched(sources, target, sems):
    rows = target.shape[0] // len(sources)
    copies = [
        pltpu.make_async_copy(source, target.at[pl.ds(k * rows, rows)], sems.at[k])
        for k, source in enumerate(sources)
    ]
    for copy in copies:
        copy.start()
    return copies


def like(shape, kind):
    return jax.ShapeDtypeStruct(shape, kind)


def exchange_lanes(left, right):
    half = LANES // 2
    lane = lax.broadcasted_iota(jnp.int32, left.shape, 1)
    low = jnp.where(lane < half, left, pltpu.roll(right, half, 1))
    high = jnp.where(lane < half, pltpu.roll(left, half, 1), right)
    return low, high


def front_kernel(copies, part, pad, *refs):
    sources, (second, out), refs = refs[:5], refs[5:7], refs[7:]
    targets, sems = refs[:5], refs[5]
    moves = [pltpu.make_async_copy(*pair, sems.at[k]) for k, pair in enumerate(zip(sources, targets))]
    for move in moves:
        move.start()
    for move in moves:
        move.wait()
    x_next, grad_out, gate, up, down_t = targets
    width = grad_out.shape[1]
    second[:, :width] = grad_out[...]
    second[:, width:] = x_next[...]
    shard, units = gate.shape
    both = jnp.concatenate((gate[...], up[...]), axis=0).astype(F32).T
    tall = jnp.concatenate((down_t[...], jnp.zeros_like(down_t))).astype(F32).T[:, :shard]
    half = pad // 2
    count = units // part
    for y in range(count):
        top = both[y * part : (y + 1) * part]
        piece = tall[y * part : (y + 1) * part]
        ahead, behind = piece[:half], piece[half:]
        behind = jnp.concatenate((behind, jnp.zeros((pad - part, shard), F32)))
        low = jnp.concatenate((ahead, behind), axis=1)
        block = jnp.concatenate((top, low)).astype(BF16)
        for z in range(copies):
            out[z * count + y] = block


def turned(array, outer, inner, rows):
    return jnp.concatenate(
        [
            array[(o * inner + i) * rows : (o * inner + i + 1) * rows]
            for i in range(inner)
            for o in range(outer)
        ]
    )


def unpack_kernel(part, pad, own, other, gate_up, down):
    half = pad // 2
    blank = jnp.zeros((pad - part, LANES), F32)
    for base, packed in ((0, own), (pad, other)):
        for tile in range(packed.shape[0] // 2):
            at = pl.ds(tile * LANES, LANES)
            low, high = exchange_lanes(packed[2 * tile].astype(F32), packed[2 * tile + 1].astype(F32))
            for row, value in ((base, low), (2 * pad + base, high)):
                gate_up[pl.ds(row, pad), at] = jnp.concatenate((value[:part], blank)).astype(BF16)
            down[pl.ds(base, half), at] = low[part:].astype(BF16)
            down[pl.ds(base + half, half), at] = high[part:].astype(BF16)


def backward_kernel(ny, nx, rows, pad, gate_up, down, prev, cotangent, kept, sent, grads):
    pre = dot(prev[...], gate_up[...], ((1,), (1,)))
    gate_prev, up_prev = pre[:, : 2 * pad], pre[:, 2 * pad :]
    grad_hidden = turned(dot(cotangent[...], down[...], ((1,), (1,))), nx, ny, rows)
    sig = jax.nn.sigmoid(gate_prev)
    silu = gate_prev * sig
    grad_gate = grad_hidden * up_prev * sig * (1.0 + gate_prev * (1.0 - sig))
    grad_up = grad_hidden * silu
    hidden_prev = turned(silu * up_prev, ny, nx, rows)
    grads[:, : 2 * pad] = grad_gate.astype(BF16)
    grads[:, 2 * pad :] = grad_up.astype(BF16)
    for k, (value, tokens) in enumerate(((grad_gate, prev), (grad_up, prev), (hidden_prev, cotangent))):
        term = dot(value.astype(BF16).T, tokens[...], ((1,), (0,)))
        kept[pl.ds(k * pad, pad)] = term[:pad]
        sent[pl.ds(k * pad, pad)] = term[pad:].astype(BF16)


def product_kernel(left, right, *outs):
    rows = outs[0].shape[0]
    for k, out in enumerate(outs):
        at = pl.ds(k * rows, rows)
        out[...] = dot(left[at, :], right[...], ((1,), (0,))).astype(BF16)


def sum_kernel(count, *refs):
    parts, outs = refs[:count], refs[count:]
    rows = outs[0].shape[0]
    total = parts[0][...].astype(F32)
    for part in parts[1:]:
        total = total + part[...].astype(F32)
    for k, out in enumerate(outs):
        out[...] = total[k * rows : (k + 1) * rows].astype(BF16)


def pair_kernel(part, pad, kept, received, out):
    half = pad // 2
    for tile in range(out.shape[0] // 2):
        at = pl.ds(tile * LANES, LANES)
        total = kept[:, at] + received[:, at].astype(F32)
        left = jnp.concatenate((total[:part], total[2 * pad : 2 * pad + half]))
        right = jnp.concatenate((total[pad : pad + part], total[2 * pad + half :]))
        even, odd = exchange_lanes(left, right)
        out[2 * tile] = even.astype(BF16)
        out[2 * tile + 1] = odd.astype(BF16)


def update_kernel(ny, part, pad, factor, arrived, gate, up, down_t, new_gate, new_up, new_down_t):
    half = pad // 2
    shard = down_t.shape[0]
    tops, lows = [], []
    for y in range(ny):
        total = arrived[y].astype(F32)
        for z in range(1, arrived.shape[0] // ny):
            total = total + arrived[z * ny + y].astype(F32)
        tops.append(total[:part])
        low = total[part:]
        lows.append(low)
        lows.append(pltpu.roll(low, LANES // 2, 1)[: part - half])
    both = jnp.concatenate(tops).T
    new_gate[...] = gate[...] + factor * both[:shard]
    new_up[...] = up[...] + factor * both[shard:]
    new_down_t[...] = down_t[...] + factor * jnp.concatenate(lows).T[:shard]


def hidden_kernel(pad, gate_up, *refs):
    pieces, (mine, theirs, hidden, tokens, sems) = refs[:-5], refs[-5:]
    for move in fetched(pieces, tokens, sems):
        move.wait()
    pre = dot(tokens[...], gate_up[...], ((1,), (1,)))
    value = jax.nn.silu(pre[:, : 2 * pad]) * pre[:, 2 * pad :]
    blank = jnp.zeros((value.shape[0], LANES - pad), F32)
    mine[...] = jnp.concatenate((value[:, :pad], blank), axis=1).astype(BF16)
    theirs[...] = jnp.concatenate((value[:, pad:], blank), axis=1).astype(BF16)
    hidden[...] = value.astype(BF16)


def middle_kernel(nx, rows, mine, partner, *refs):
    parts, outs = refs[:nx], refs[nx:]
    ny, width = len(outs), parts[0].shape[1]
    total = parts[0][...].astype(F32)
    for part in parts[1:]:
        total = total + part[...].astype(F32)
    own, other = mine[...].astype(F32), partner[...].astype(F32)
    for k, out in enumerate(outs):
        out[:, :width] = total[k * rows : (k + 1) * rows].astype(BF16)
        for x in range(nx):
            at, lane = (x * ny + k) * rows, width + 2 * LANES * x
            out[:, lane : lane + LANES] = own[at : at + rows].astype(BF16)
            out[:, lane + LANES : lane + 2 * LANES] = other[at : at + rows].astype(BF16)


def arrival_kernel(nx, part, place, *refs):
    parts, (output, saved, by_y, by_x) = refs[:-4], refs[-4:]
    ny, (rows, width) = len(parts), output.shape
    total = parts[0][:, :width].astype(F32)
    for piece in parts[1:]:
        total = total + piece[:, :width].astype(F32)
    output[...] = total.astype(BF16)
    x, y, core = place[0], place[1], place[2]
    for k in range(ny):
        by_y[k] = parts[k][:, width:].astype(F32)
    pieces = [by_y[lax.rem(y - s + ny, ny)] for s in range(ny)]
    for k in range(nx):
        lane = 2 * LANES * k
        here = jnp.concatenate([piece[:, lane : lane + part] for piece in pieces], axis=1)
        lane = lane + LANES
        there = jnp.concatenate([piece[:, lane : lane + part] for piece in pieces], axis=1)
        by_x[k, :rows] = jnp.where(core == 0, here, there)
        by_x[k, rows:] = jnp.where(core == 0, there, here)
    ordered = [by_x[lax.rem(s - x + nx, nx)] for s in range(nx)]
    saved[...] = jnp.concatenate(ordered).astype(BF16)


def layer(x_next, x_prev, grad_out, gate_w, up_w, down_w, acc_gate, acc_up, acc_down):
    rows, width = x_prev.shape
    nz, ny, nx, nc = (lax.axis_size(name) for name in ALL)
    group = ny * nx * rows
    factor = 1.0 / math.sqrt(rows * nz * ny * nx * nc)
    units = gate_w.shape[1]
    part = units // ny
    pad = -(-part // 32) * 32
    block = (nz * ny, part + pad // 2, LANES)
    token_ops = 2 * group * 2 * pad * width

    second, packed = whole(
        functools.partial(front_kernel, nz, part, pad),
        (like((rows, 2 * width), BF16), like(block, BF16)),
        (x_next, grad_out, gate_w, up_w, down_w.T),
        (
            *(pltpu.VMEM((rows, width), BF16) for _ in range(2)),
            *(pltpu.VMEM((width // (nz * ny), units), BF16) for _ in range(3)),
            pltpu.SemaphoreType.DMA((5,)),
        ),
        grant=60,
        spaces=[pltpu.HBM] * 5,
        result=None,
    )

    own = spread(packed, FS)
    other = swapped(own)

    first = jnp.stack(around(x_prev, "x")).reshape(nx * rows, width)
    second = jnp.stack(around(second, "y")).reshape(ny * rows, 2 * width)
    prevs = around(first, "y")
    cotangents = around(second[:, :width], "x")
    nexts = around(second[:, width:], "x")
    gate_up, down = whole(
        functools.partial(unpack_kernel, part, pad),
        (like((4 * pad, width), BF16), like((2 * pad, width), BF16)),
        (own, other),
    )

    prev = jnp.concatenate(prevs)
    cotangent = jnp.concatenate(cotangents)
    kept, sent, grads = whole(
        functools.partial(backward_kernel, ny, nx, rows, pad),
        (like((3 * pad, width), F32), like((3 * pad, width), BF16), like((group, 4 * pad), BF16)),
        (gate_up, down, prev, cotangent),
        flops=6 * token_ops,
    )
    received = swapped(sent)
    input_parts = whole(
        product_kernel,
        tuple(like((nx * rows, width), BF16) for _ in range(ny)),
        (grads, gate_up),
        flops=2 * token_ops,
    )
    paired = whole(functools.partial(pair_kernel, part, pad), like(block, BF16), (kept, received))
    arrived = spread(paired, FS)
    new_gate, new_up, new_down_t = whole(
        functools.partial(update_kernel, ny, part, pad, factor),
        (like(acc_gate.shape, F32), like(acc_up.shape, F32), like(acc_down.shape[::-1], F32)),
        (arrived, acc_gate, acc_up, acc_down.T),
    )

    arrivals = for_owner(input_parts, "y")
    by_y = whole(
        functools.partial(sum_kernel, ny),
        tuple(like((rows, width), BF16) for _ in range(nx)),
        arrivals,
    )
    grad_input = added(for_owner(by_y, "x"))

    mine, theirs, hidden = whole(
        functools.partial(hidden_kernel, pad),
        (like((group, LANES), BF16), like((group, LANES), BF16), like((group, 2 * pad), BF16)),
        (gate_up, *nexts),
        (pltpu.VMEM((group, width), BF16), pltpu.SemaphoreType.DMA((nx,))),
        flops=2 * token_ops,
        spaces=[pltpu.VMEM] + [pltpu.HBM] * nx,
    )
    partner = swapped(theirs)
    out_parts = whole(
        product_kernel,
        tuple(like((ny * rows, width), BF16) for _ in range(nx)),
        (hidden, down),
        flops=token_ops,
    )
    arrivals = for_owner(out_parts, "x")
    by_x = whole(
        functools.partial(middle_kernel, nx, rows),
        tuple(like((rows, width + 2 * nx * LANES), BF16) for _ in range(ny)),
        (mine, partner, *arrivals),
    )
    arrivals = for_owner(by_x, "y")
    place = jnp.stack([lax.axis_index(name) for name in ("x", "y", "c")]).astype(jnp.int32)
    out_next, saved = whole(
        functools.partial(arrival_kernel, nx, part),
        (like((rows, width), BF16), like((nx * nc * rows, units), BF16)),
        (place, *arrivals),
        (
            pltpu.VMEM((ny, rows, 2 * nx * LANES), F32),
            pltpu.VMEM((nx, nc * rows, units), F32),
        ),
        spaces=[pltpu.SMEM] + [pltpu.VMEM] * ny,
    )
    return out_next, saved, grad_input, new_gate, new_up, new_down_t.T


def solution(mesh):
    split = Mesh(mesh.devices.reshape(8, 4, 4, 2), ALL)
    tokens = P(ALL, None)
    wide, tall = P(FS, TP), P(TP, FS)
    in_specs = (tokens, tokens, tokens, wide, wide, tall, wide, wide, tall)
    out_specs = (tokens, wide, tokens, wide, wide, tall)
    return jax.shard_map(layer, mesh=split, in_specs=in_specs, out_specs=out_specs, check_vma=False)
```
